256 devices in a mesh: sp: 64 (over z, x, core), tp: 4 (over y).
Axes of the slice: x: 4, y: 4, z: 8, core: 2. Of those that a mesh axis runs over, the one named last changes fastest.
Arguments:
- stream: bfloat16 [32768, 2048], P(('sp', 'tp')), may hold values from -6 to 6
- queries: bfloat16 [32768, 512], P('sp', 'tp'), may hold values from -6 to 6
- key_rows: bfloat16 [32768, 512], P('sp', 'tp'), may hold values from -6 to 6
- values: bfloat16 [32768, 1024], P('sp', 'tp'), may hold values from -6 to 6
- out_gate: bfloat16 [32768, 1024], P('sp', 'tp'), may hold values from -6 to 6
- fwd_decay: float32 [32768, 512], P('sp', 'tp'), may hold values from -14 to 14
- bwd_decay: float32 [32768, 512], P('sp', 'tp'), may hold values from -14 to 14
- head_gain: float32 [1024], P('tp'), may hold values from 0.1 to 1.9
- out_proj: bfloat16 [1024, 2048], replicated, may hold values from -0.1875 to 0.1875
- mix_gain: float32 [2048], replicated, may hold values from 0.1 to 1.9
- ffn_gain: float32 [2048], replicated, may hold values from 0.1 to 1.9
- moe_gain: float32 [2048], replicated, may hold values from 0.1 to 1.9
- routes: int32 [32768, 2], P(('sp', 'tp')), may hold values from 0 to 63, all different within a row; in each aligned block of 128 rows (0 to 127, 128 to 255, ...) at most 6 rows name the same one
- route_weight: float32 [32768, 2], P(('sp', 'tp')), may hold values from 0.25 to 2.5
- expert_gate: bfloat16 [64, 2048, 1024], P('sp', None, 'tp'), may hold values from -0.125 to 0.125
- expert_up: bfloat16 [64, 2048, 1024], P('sp', None, 'tp'), may hold values from -0.125 to 0.125
- expert_down: bfloat16 [64, 1024, 2048], P('sp', 'tp'), may hold values from -0.1875 to 0.1875
- shared_gate: bfloat16 [2048, 512], P(None, 'tp'), may hold values from -0.125 to 0.125
- shared_up: bfloat16 [2048, 512], P(None, 'tp'), may hold values from -0.125 to 0.125
- shared_down: bfloat16 [512, 2048], P('tp'), may hold values from -0.25 to 0.25
Outputs:
- updated: bfloat16 [32768, 2048], P(('sp', 'tp'))
The draws below stay inside these ranges and needn't reach their ends.
Inputs may be any that keep to these rules, and one draw needn't show every extreme that they name: `routes`: each row names 2 different experts. Among the rows of one device no expert is named more than 6 times, and in every draw some device names some expert exactly 6 times.
All inputs are finite; a program needn't handle non-finite values.
Results may differ from the reference program's by a relative error of at most 0.023.
Values may be sent and summed in bfloat16 or wider, within the bound.
A program may use at most 128 MiB of HBM per device.

```python
import math
import jax
import jax.numpy as jnp
import numpy as np
from jax import lax

D = 2048
HEAD_TOTAL = 8
KEY_CHANNELS = 64
DV = 128
BLK = 64
FE = 1024
SH = 512
TOPK = 2
TOK_DEV = 128
TOKEN_COUNT = 32768
HV = 1024
EXPERTS = 64
CAP = 6
PARTS_SIZE = 4


def decay_law(key):
    head_key, chan_key, dev_key, jitter_key, position_key, fraction_key = jax.random.split(key, 6)
    slow_share = 0.5
    slow_heads = jax.random.uniform(head_key, (HEAD_TOTAL,)) < slow_share
    head_rate = jnp.where(slow_heads, 0.6 / TOKEN_COUNT, 2.5 / BLK)
    channel_rate = jnp.repeat(head_rate, KEY_CHANNELS) * jnp.exp(jax.random.uniform(chan_key, (HEAD_TOTAL * KEY_CHANNELS,), minval=-0.5, maxval=0.5))
    device_factor = jnp.exp(jax.random.uniform(dev_key, (TOKEN_COUNT // TOK_DEV, 1), minval=-0.7, maxval=0.7))
    rates = jnp.repeat(device_factor, TOK_DEV, axis=0) * channel_rate[None, :]
    preactivation = -jnp.log(jnp.expm1(16.0 * rates))
    preactivation = preactivation + jax.random.uniform(jitter_key, (TOKEN_COUNT, HEAD_TOTAL * KEY_CHANNELS), minval=-1.0, maxval=1.0)
    spike_rows = jax.random.randint(position_key, (2,), 0, TOKEN_COUNT)
    spike_fraction = jax.random.uniform(fraction_key, (2, HEAD_TOTAL * KEY_CHANNELS), minval=0.2, maxval=0.5)
    spike_preactivation = -jnp.log(jnp.expm1(-16.0 * jnp.log(1.0 - spike_fraction)))
    preactivation = preactivation.at[spike_rows].set(spike_preactivation)
    return jnp.clip(preactivation, -14.0, 14.0).astype(jnp.float32)


def draw_fwd_decay(key, part):
    return decay_law(jax.random.fold_in(key, 11))


def draw_bwd_decay(key, part):
    return decay_law(jax.random.fold_in(key, 23))


def levels(own_key, dims, cuts, low, high):
    gain = 1.0
    for dim, blocks in cuts:
        draws = jax.random.uniform(jax.random.fold_in(jax.random.fold_in(own_key, 6), dim), (blocks,), jnp.float32, low / len(cuts), high / len(cuts))
        gain = gain * jnp.repeat(jnp.exp(draws), dims[dim] // blocks).reshape((-1,) + (1,) * (len(dims) - 1 - dim))
    return gain


def deal_out(key, own, number, rows, amount, top, most, lean):
    sequence = jax.random.permutation(key, amount)
    heavy_load, ordinary = portions_of(amount, rows * top, most, lean, True), portions_of(amount, rows * top, most, lean, False)
    places = jnp.arange(amount)

    def named(tallies, rotation):
        used = int((tallies > 0).sum())
        fixed = max(1, used // 4)
        shifted = fixed + (places - fixed + rotation * (used - fixed)) % max(1, amount - fixed)
        return jnp.zeros((amount,), jnp.int32).at[sequence[jnp.where(places < fixed, places, shifted)]].set(jnp.asarray(tallies, jnp.int32))

    tallies = jnp.where(number % 4 == 0, named(heavy_load, number // 4), named(ordinary, number - number // 4 - 1))
    mixed = jax.random.permutation(jax.random.fold_in(own, 3), amount)
    giver, taker = mixed[0:amount // 2 * 2:2], mixed[1:amount // 2 * 2:2]
    room = jnp.minimum(tallies[giver] - 1, most - tallies[taker]) // 2
    room = jnp.where((giver == sequence[0]) | (taker == sequence[0]) | (tallies[taker] == 0), 0, jnp.maximum(room, 0))
    shifted = jax.random.randint(jax.random.fold_in(own, 4), (amount // 2,), 0, 1 << 20) % (room + 1)
    tallies = tallies.at[giver].add(-shifted).at[taker].add(shifted)
    members = jnp.searchsorted(jnp.cumsum(tallies), jnp.arange(rows * top), side="right").astype(jnp.int32)
    listing = members.reshape(top, rows).T
    listing = listing[jax.random.permutation(jax.random.fold_in(own, 1), rows)]
    rotation = jax.random.randint(jax.random.fold_in(own, 2), (rows, 1), 0, top)
    return jnp.take_along_axis(listing, (jnp.arange(top)[None, :] + rotation) % top, axis=1)


def portions_of(count, total, reach, skew, full):
    weights = [(1 << 20) // math.isqrt(standing ** skew) + 1 for standing in range(1, count + 1)]
    largest = reach if full else min(reach, max(-(-total // count), total * weights[0] // sum(weights)))
    least = 1 if total - largest >= count - 1 else 0
    given, surplus = [largest] + [least] * (count - 1), total - largest - least * (count - 1)
    while surplus > 0:
        free = [i for i in range(1, count) if given[i] < largest] or [i for i in range(1, count) if given[i] < reach]
        mass, left = sum([weights[i] for i in free]), surplus
        for i in free:
            extra = min(reach - given[i], max(1, left * weights[i] // mass), surplus)
            given[i] = given[i] + extra
            surplus = surplus - extra
    return np.array(given)


def bell_draw(own_key, dims, width, most, cuts=(), kind=jnp.bfloat16):
    drawn = jax.random.normal(own_key, dims, jnp.float32) * width
    if len(cuts) > 0:
        drawn = levels(own_key, dims, cuts, -0.22, 0.18) * drawn
    return jnp.clip(drawn, min=-most, max=most).astype(kind)


def setup_inputs(seed: int = 0) -> dict:
    arg_keys = jax.random.split(jax.random.key(seed), 21)
    stream = bell_draw(arg_keys[0], (TOKEN_COUNT, D), 1.0, 6.0, ((0, 256),))
    queries = bell_draw(arg_keys[1], (TOKEN_COUNT, HEAD_TOTAL * KEY_CHANNELS), 1.0, 6.0, ((0, 64), (1, 4)))
    key_rows = bell_draw(arg_keys[2], (TOKEN_COUNT, HEAD_TOTAL * KEY_CHANNELS), 1.0, 6.0, ((0, 64), (1, 4)))
    values = bell_draw(arg_keys[3], (TOKEN_COUNT, HV), 1.0, 6.0, ((0, 64), (1, 4)))
    out_gate = bell_draw(arg_keys[4], (TOKEN_COUNT, HV), 1.0, 6.0, ((0, 64), (1, 4)))
    fwd_decay = draw_fwd_decay(jax.random.fold_in(arg_keys[20], 71), 0)
    bwd_decay = draw_bwd_decay(jax.random.fold_in(arg_keys[20], 71), 0)
    head_gain = jnp.clip(1.0 + 0.18 * jax.random.normal(arg_keys[7], (HV,), jnp.float32), 0.1, 1.9)
    out_proj = bell_draw(arg_keys[8], (HV, D), HV ** -0.5, 0.1875)
    mix_gain = jnp.clip(1.0 + 0.18 * jax.random.normal(arg_keys[9], (D,), jnp.float32), 0.1, 1.9)
    ffn_gain = jnp.clip(1.0 + 0.18 * jax.random.normal(arg_keys[10], (D,), jnp.float32), 0.1, 1.9)
    moe_gain = jnp.clip(1.0 + 0.18 * jax.random.normal(arg_keys[11], (D,), jnp.float32), 0.1, 1.9)
    routes_keys = jax.random.split(jax.random.fold_in(arg_keys[12], 1), TOKEN_COUNT // TOK_DEV)
    routes_turns = jax.random.permutation(jax.random.fold_in(arg_keys[12], 3), TOKEN_COUNT // TOK_DEV)
    routes = jax.vmap(lambda own, number: deal_out(jax.random.fold_in(arg_keys[12], 2), own, number, TOK_DEV, EXPERTS, TOPK, CAP, 1))(routes_keys, routes_turns).reshape((TOKEN_COUNT, TOPK))
    route_weight = jnp.clip(jnp.exp(math.log(2.5) - 2.3025851 * jax.random.uniform(arg_keys[13], (TOKEN_COUNT, TOPK), jnp.float32) ** levels(arg_keys[13], (TOKEN_COUNT, TOPK), ((0, 256),), -0.2, 0.2)), 0.25, 2.5)
    expert_gate = bell_draw(arg_keys[14], (EXPERTS, D, FE), D ** -0.5, 0.125, ((0, 64), (2, 4)))
    expert_up = bell_draw(arg_keys[15], (EXPERTS, D, FE), D ** -0.5, 0.125, ((0, 64), (2, 4)))
    expert_down = bell_draw(arg_keys[16], (EXPERTS, FE, D), FE ** -0.5, 0.1875, ((0, 64), (1, 4)))
    shared_gate = bell_draw(arg_keys[17], (D, SH), D ** -0.5, 0.125, ((1, 4),))
    shared_up = bell_draw(arg_keys[18], (D, SH), D ** -0.5, 0.125, ((1, 4),))
    shared_down = bell_draw(arg_keys[19], (SH, D), SH ** -0.5, 0.25, ((0, 4),))
    return {"stream": stream, "queries": queries, "key_rows": key_rows, "values": values, "out_gate": out_gate, "fwd_decay": fwd_decay, "bwd_decay": bwd_decay, "head_gain": head_gain, "out_proj": out_proj, "mix_gain": mix_gain, "ffn_gain": ffn_gain, "moe_gain": moe_gain, "routes": routes, "route_weight": route_weight, "expert_gate": expert_gate, "expert_up": expert_up, "expert_down": expert_down, "shared_gate": shared_gate, "shared_up": shared_up, "shared_down": shared_down}


EPS = 1e-06
GATE_NORM = 16.0
ROPE_BASE = 10000.0
TOP_PRECISION = lax.Precision.HIGHEST

def normalize(tensor):
    return tensor * lax.rsqrt(lax.optimization_barrier(jnp.mean(tensor * tensor, axis=-1, keepdims=True)) + EPS)

def rotate(tensor, positions):
    half_width = tensor.shape[-1] // 2
    frequency = ROPE_BASE ** (-jnp.arange(half_width, dtype=jnp.float32) / half_width)
    angles = positions[:, None] * frequency[None, :]
    cosine = jnp.cos(angles)[:, None, :]
    sine_part = jnp.sin(angles)[:, None, :]
    front_half = tensor[..., :half_width]
    back_half = tensor[..., half_width:]
    return jnp.concatenate([front_half * cosine - back_half * sine_part, front_half * sine_part + back_half * cosine], axis=-1)

def blockwise(query_rows, key_data, value_matrix, log_decay, start_state):
    length, head_count, key_width = query_rows.shape
    value_width = value_matrix.shape[-1]
    block_count = length // BLK
    query_blocks = query_rows.reshape(block_count, BLK, head_count, key_width)
    key_blocks = key_data.reshape(block_count, BLK, head_count, key_width)
    value_blocks = value_matrix.reshape(block_count, BLK, head_count, value_width)
    cumul = jnp.cumsum(log_decay.reshape(block_count, BLK, head_count, key_width), axis=1)
    middle = cumul[:, BLK // 2 - 1:BLK // 2]
    query_scaled = query_blocks * jnp.exp(cumul - middle)
    key_scaled = key_blocks * jnp.exp(middle - cumul)
    scores = jnp.einsum('nthk,nshk->nhts', query_scaled, key_scaled, precision=TOP_PRECISION)
    lower_mask = jnp.arange(BLK)[:, None] >= jnp.arange(BLK)[None, :]
    scores = jnp.where(lower_mask, scores, 0.0)
    within = jnp.einsum('nhts,nshv->nthv', scores, value_blocks, precision=TOP_PRECISION)
    last_cumul = cumul[:, -1:]
    query_in = query_blocks * jnp.exp(cumul)
    key_out = key_blocks * jnp.exp(last_cumul - cumul)
    block_decay = jnp.exp(last_cumul[:, 0])

    def advance(carried_state, pieces):
        query_segment, key_segment, value_segment, decay_segment = pieces
        across_blocks = jnp.einsum('asu,sun->asn', query_segment, carried_state, precision=TOP_PRECISION)
        carried_state = carried_state * decay_segment[:, :, None] + jnp.einsum('jco,jcm->com', key_segment, value_segment, precision=TOP_PRECISION)
        return (carried_state, across_blocks)
    final_state, across_blocks = lax.scan(advance, start_state, (query_in, key_out, value_blocks, block_decay))
    return ((within + across_blocks).reshape(length, head_count, value_width), final_state)

def reference(stream, queries, key_rows, values, out_gate, fwd_decay, bwd_decay, head_gain, out_proj, mix_gain, ffn_gain, moe_gain, routes, route_weight, expert_gate, expert_up, expert_down, shared_gate, shared_up, shared_down):
    positions = jnp.arange(TOKEN_COUNT, dtype=jnp.int32).astype(jnp.float32)
    query_rows = rotate(queries.astype(jnp.float32).reshape(TOKEN_COUNT, HEAD_TOTAL, KEY_CHANNELS) * KEY_CHANNELS ** (-0.5), positions)
    key_data = rotate(key_rows.astype(jnp.float32).reshape(TOKEN_COUNT, HEAD_TOTAL, KEY_CHANNELS), positions)
    value_matrix = values.astype(jnp.float32).reshape(TOKEN_COUNT, HEAD_TOTAL, DV)
    fwd_log = jax.nn.log_sigmoid(fwd_decay).reshape(TOKEN_COUNT, HEAD_TOTAL, KEY_CHANNELS) / GATE_NORM
    bwd_log = jax.nn.log_sigmoid(bwd_decay).reshape(TOKEN_COUNT, HEAD_TOTAL, KEY_CHANNELS) / GATE_NORM
    zero_state = jnp.zeros((HEAD_TOTAL, KEY_CHANNELS, DV), jnp.float32)
    fwd_out, _ = blockwise(query_rows, key_data, value_matrix, fwd_log, zero_state)
    bwd_out, _ = blockwise(query_rows[::-1], key_data[::-1], value_matrix[::-1], bwd_log[::-1], zero_state)
    combined = normalize(fwd_out + bwd_out[::-1]) * head_gain.reshape(HEAD_TOTAL, DV)
    mixed_out = (combined.reshape(TOKEN_COUNT, HV) * jax.nn.silu(out_gate.astype(jnp.float32))).astype(jnp.bfloat16)
    projected = jnp.dot(mixed_out, out_proj, preferred_element_type=jnp.float32)
    residual = (stream.astype(jnp.float32) + normalize(projected) * mix_gain).astype(jnp.bfloat16)
    normed = (normalize(residual.astype(jnp.float32)) * ffn_gain).astype(jnp.bfloat16)
    shared_hidden = (jax.nn.silu(jnp.dot(normed, shared_gate, preferred_element_type=jnp.float32)) * jnp.dot(normed, shared_up, preferred_element_type=jnp.float32)).astype(jnp.bfloat16)
    group_width = SH // PARTS_SIZE
    shared_out = jnp.zeros((TOKEN_COUNT, D), jnp.float32)
    for quarter in range(PARTS_SIZE):
        piece = jnp.dot(shared_hidden[:, quarter * group_width:(quarter + 1) * group_width], shared_down[quarter * group_width:(quarter + 1) * group_width], preferred_element_type=jnp.float32)
        shared_out = shared_out + lax.optimization_barrier(piece.astype(jnp.bfloat16)).astype(jnp.float32)
    row_block = 256
    flat_ids = routes.reshape(-1)
    grand_total = flat_ids.shape[0]
    token_index = jnp.arange(grand_total, dtype=jnp.int32) // TOPK
    sort_order = jnp.argsort(flat_ids, stable=True)
    sorted_expert = flat_ids[sort_order]
    sorted_token = token_index[sort_order]
    sorted_weight = route_weight.reshape(-1)[sort_order]
    counts = lax.optimization_barrier(jnp.sum((flat_ids[:, None] == jnp.arange(EXPERTS, dtype=jnp.int32)[None, :]).astype(jnp.int32), axis=0))
    starts = jnp.cumsum(counts) - counts
    padded = (counts + row_block - 1) // row_block * row_block
    block_ends = jnp.cumsum(padded)
    padded_starts = block_ends - padded
    position = (padded_starts[sorted_expert] + jnp.arange(grand_total, dtype=jnp.int32) - starts[sorted_expert]).astype(jnp.int32)
    block_total = -(-(grand_total + EXPERTS * (row_block - 1)) // row_block)
    slot_token = jnp.zeros((block_total * row_block,), jnp.int32).at[position].set(sorted_token)
    slot_weight = jnp.zeros((block_total * row_block,), jnp.float32).at[position].set(sorted_weight)
    block_expert = jnp.minimum(jnp.searchsorted(block_ends, jnp.arange(block_total, dtype=jnp.int32) * row_block, side='right'), EXPERTS - 1).astype(jnp.int32)
    expert_width = FE // PARTS_SIZE

    def add_block(totals, block_item):
        token_ids, slot_wts, expert = block_item
        row_data = normed[token_ids]
        gate_mat = lax.dynamic_index_in_dim(expert_gate, expert, 0, keepdims=False)
        up_mat = lax.dynamic_index_in_dim(expert_up, expert, 0, keepdims=False)
        down_mat = lax.dynamic_index_in_dim(expert_down, expert, 0, keepdims=False)
        hidden = (jax.nn.silu(jnp.dot(row_data, gate_mat, preferred_element_type=jnp.float32)) * jnp.dot(row_data, up_mat, preferred_element_type=jnp.float32)).astype(jnp.bfloat16)
        quarter_sums = jnp.einsum('rqf,qfd->qrd', hidden.astype(jnp.float32).reshape(row_block, PARTS_SIZE, expert_width), down_mat.astype(jnp.float32).reshape(PARTS_SIZE, expert_width, D), precision=TOP_PRECISION)
        rounded = lax.optimization_barrier(quarter_sums.astype(jnp.bfloat16)).astype(jnp.float32)
        result = lax.optimization_barrier(lax.optimization_barrier(jnp.sum(rounded, axis=0)).astype(jnp.bfloat16)).astype(jnp.float32)
        return (totals.at[token_ids].add(result * slot_wts[:, None]), None)
    routed_sum, _ = lax.scan(add_block, jnp.zeros((TOKEN_COUNT, D), jnp.float32), (slot_token.reshape(block_total, row_block), slot_weight.reshape(block_total, row_block), block_expert))
    mixture = shared_out + routed_sum
    return (residual.astype(jnp.float32) + normalize(mixture) * moe_gain).astype(jnp.bfloat16)
```

```python
import functools

import jax
import jax.numpy as jnp
import numpy as np
from jax import lax
from jax.experimental import pallas as pl
from jax.experimental.pallas import tpu as pltpu
from jax.sharding import PartitionSpec as P

KEY_CHANNELS = 64
DV = 128
TOPK = 2
CAP = 6
CHUNK = 128
LANES = 128
EPS = 1e-06
GATE_NORM = 16.0
ROPE_BASE = 10000.0
MESH = pl.DeviceIdType.MESH
NT = (((1,), (1,)), ((), ()))
TN = (((0,), (0,)), ((), ()))
F32 = jnp.float32
BF16 = jnp.bfloat16


def rope_tables(span, devices):
    half = KEY_CHANNELS // 2
    freq = ROPE_BASE ** (-np.arange(half, dtype=np.float64) / half)
    freq = np.tile(freq, LANES // half)
    inner = np.arange(span)[:, None] * freq[None, :]
    outer = (np.arange(devices) * span)[:, None] * freq[None, :]
    inner = np.stack([np.cos(inner), np.sin(inner)]).astype(np.float32)
    outer = np.stack([np.cos(outer), np.sin(outer)], axis=1).astype(np.float32)
    return inner, outer


def attention_kernel(
    groups,
    members,
    q_ref,
    k_ref,
    v_ref,
    g_ref,
    fd_ref,
    bd_ref,
    gain_ref,
    inner_ref,
    outer_ref,
    mixed_ref,
    qs_ref,
    ks_ref,
    out_ref,
    upd_ref,
    half_ref,
    send_ref,
    got_ref,
    back_ref,
    carry_ref,
    mine_ref,
    send_sem,
    recv_sem,
    back_send_sem,
    back_recv_sem,
    mix_send_sem,
    mix_recv_sem,
):
    me = lax.axis_index("sp")
    row = lax.axis_index("tp")
    span = q_ref.shape[0]
    chunks = span // CHUNK
    share = DV // groups
    message = 4 * share

    barrier = pltpu.get_barrier_semaphore()

    def greet(i, c):
        pl.semaphore_signal(
            barrier, inc=1, device_id={"sp": lax.rem(me + i, groups)}, device_id_type=MESH
        )
        return c

    lax.fori_loop(1, groups, greet, 0)
    for i in range(1, members):
        pl.semaphore_signal(
            barrier, inc=1, device_id={"tp": lax.rem(row + i, members)}, device_id_type=MESH
        )

    lane = lax.broadcasted_iota(jnp.int32, (CHUNK, LANES), 1)
    r_id = lax.broadcasted_iota(jnp.int32, (CHUNK, CHUNK), 0)
    c_id = lax.broadcasted_iota(jnp.int32, (CHUNK, CHUNK), 1)
    lower = r_id >= c_id
    upper = r_id <= c_id
    lower_one = jnp.where(lower, 1.0, 0.0).astype(BF16)
    upper_one = jnp.where(upper, 1.0, 0.0).astype(BF16)
    front = (lane % KEY_CHANNELS) < (KEY_CHANNELS // 2)
    first_head = lane < KEY_CHANNELS
    cos_0 = outer_ref[0:1, :]
    sin_0 = outer_ref[1:2, :]

    def log_decay(x):
        return (jnp.minimum(x, 0.0) - jnp.log1p(jnp.exp(-jnp.abs(x)))) * (1.0 / GATE_NORM)

    def cumulate(tri, x):
        high = x.astype(BF16)
        low = (x - high.astype(F32)).astype(BF16)
        return jnp.dot(tri, high, preferred_element_type=F32) + jnp.dot(
            tri, low, preferred_element_type=F32
        )

    for b in range(chunks):
        rows = slice(b * CHUNK, (b + 1) * CHUNK)
        cos_i = inner_ref[0, rows, :]
        sin_i = inner_ref[1, rows, :]
        cosine = cos_0 * cos_i - sin_0 * sin_i
        sine = sin_0 * cos_i + cos_0 * sin_i
        sine = jnp.where(front, -sine, sine)

        def rotated(u):
            swapped = jnp.where(
                front,
                pltpu.roll(u, LANES - KEY_CHANNELS // 2, 1),
                pltpu.roll(u, KEY_CHANNELS // 2, 1),
            )
            return u * cosine + swapped * sine

        q = rotated(q_ref[rows, :].astype(F32) * KEY_CHANNELS ** (-0.5))
        k = rotated(k_ref[rows, :].astype(F32))
        cf = cumulate(lower_one, log_decay(fd_ref[rows, :]))
        cb = cumulate(upper_one, log_decay(bd_ref[rows, :]))
        hf = cf[CHUNK - 1 : CHUNK, :] * 0.5
        hb = cb[0:1, :] * 0.5
        half_ref[2 * b : 2 * b + 1, :] = hf
        half_ref[2 * b + 1 : 2 * b + 2, :] = hb
        qf = q * jnp.exp(cf - hf)
        qb = q * jnp.exp(cb - hb)
        kf = (k * jnp.exp(hf - cf)).astype(BF16)
        kb = (k * jnp.exp(hb - cb)).astype(BF16)
        ks_ref[b, :, 0:LANES] = kf
        ks_ref[b, :, LANES : 2 * LANES] = kb
        qs_ref[b, 0:CHUNK, 0:LANES] = jnp.where(first_head, qf, 0.0).astype(BF16)
        qs_ref[b, 0:CHUNK, LANES : 2 * LANES] = jnp.where(first_head, qb, 0.0).astype(BF16)
        qs_ref[b, CHUNK : 2 * CHUNK, 0:LANES] = jnp.where(first_head, 0.0, qf).astype(BF16)
        qs_ref[b, CHUNK : 2 * CHUNK, LANES : 2 * LANES] = jnp.where(first_head, 0.0, qb).astype(
            BF16
        )
        both = lax.dot_general(
            v_ref[rows, :], ks_ref[b], TN, preferred_element_type=F32
        )
        upd_ref[2 * b] = jnp.where(
            first_head, both[0:DV, 0:LANES], both[DV : 2 * DV, 0:LANES]
        ) * jnp.exp(hf)
        upd_ref[2 * b + 1] = jnp.where(
            first_head, both[0:DV, LANES : 2 * LANES], both[DV : 2 * DV, LANES : 2 * LANES]
        ) * jnp.exp(hb)

    def decay_of(b, d):
        return jnp.exp(half_ref[2 * b + d : 2 * b + d + 1, :] * 2.0)

    total_f = upd_ref[0]
    decay_f = decay_of(0, 0)
    for b in range(1, chunks):
        total_f = total_f * decay_of(b, 0) + upd_ref[2 * b]
        decay_f = decay_f * decay_of(b, 0)
    total_b = upd_ref[2 * (chunks - 1) + 1]
    decay_b = decay_of(chunks - 1, 1)
    for b in reversed(range(chunks - 1)):
        total_b = total_b * decay_of(b, 1) + upd_ref[2 * b + 1]
        decay_b = decay_b * decay_of(b, 1)
    for r in range(share):
        part = slice(r * groups, (r + 1) * groups)
        send_ref[pl.ds(r, groups, stride=message), :] = total_f[part, :]
        send_ref[pl.ds(share + r, groups, stride=message), :] = total_b[part, :]
        send_ref[pl.ds(2 * share + r, groups, stride=message), :] = jnp.broadcast_to(
            decay_f, (groups, LANES)
        )
        send_ref[pl.ds(3 * share + r, groups, stride=message), :] = jnp.broadcast_to(
            decay_b, (groups, LANES)
        )

    pl.semaphore_wait(barrier, groups - 1 + members - 1)

    def block(ref, i):
        return ref.at[pl.ds(pl.multiple_of(i * message, message), message)]

    def half_block(ref, i):
        return ref.at[i]

    def out_copy(peer, i):
        return pltpu.make_async_remote_copy(
            src_ref=block(send_ref, peer),
            dst_ref=block(got_ref, me),
            send_sem=send_sem.at[i],
            recv_sem=recv_sem.at[i],
            device_id={"sp": peer},
            device_id_type=MESH,
        )

    def back_copy(peer, i):
        return pltpu.make_async_remote_copy(
            src_ref=half_block(back_ref, peer),
            dst_ref=half_block(carry_ref, me),
            send_sem=back_send_sem.at[i],
            recv_sem=back_recv_sem.at[i],
            device_id={"sp": peer},
            device_id_type=MESH,
        )

    def offset(i):
        half = lax.div(i + 1, 2)
        return jnp.where(lax.rem(i, 2) == 1, half, groups - half)

    def peer_of(i):
        return lax.rem(me + offset(i), groups)

    def each(action):
        def step(i, c):
            action(i)
            return c

        lax.fori_loop(1, groups, step, 0)

    each(lambda i: out_copy(peer_of(i), offset(i)).start())
    mine = pl.ds(pl.multiple_of(me * message, message), message)
    got_ref[mine, :] = send_ref[mine, :]

    for b in range(chunks):
        rows = slice(b * CHUNK, (b + 1) * CHUNK)
        s_f = lax.dot_general(
            qs_ref[b, :, 0:LANES], ks_ref[b, :, 0:LANES], NT, preferred_element_type=F32
        )
        s_b = lax.dot_general(
            qs_ref[b, :, LANES : 2 * LANES],
            ks_ref[b, :, LANES : 2 * LANES],
            NT,
            preferred_element_type=F32,
        )
        for h in range(2):
            part = slice(h * CHUNK, (h + 1) * CHUNK)
            s = jnp.where(lower, s_f[part], 0.0) + jnp.where(upper, s_b[part], 0.0)
            out_ref[h, rows, :] = jnp.dot(
                s.astype(BF16), v_ref[rows, h * DV : (h + 1) * DV], preferred_element_type=F32
            )

    each(lambda i: out_copy(peer_of(i), offset(i)).wait())

    zero = jnp.zeros((share, LANES), F32)

    def scan(s, carried):
        c_f, c_b = carried
        t = groups - 1 - s
        at_s = pl.multiple_of(s * message, message)
        at_t = pl.multiple_of(t * message, message)
        m_s = got_ref[pl.ds(at_s, message), :]
        m_t = got_ref[pl.ds(at_t, message), :]
        back_ref[s, 0:share, :] = c_f
        back_ref[t, share : 2 * share, :] = c_b
        c_f = c_f * m_s[2 * share : 3 * share] + m_s[0:share]
        c_b = c_b * m_t[3 * share : 4 * share] + m_t[share : 2 * share]
        return c_f, c_b

    lax.fori_loop(0, groups, scan, (zero, zero))
    each(lambda i: back_copy(peer_of(i), offset(i)).start())
    carry_ref[me] = back_ref[me]
    each(lambda i: back_copy(peer_of(i), offset(i)).wait())

    state_f = jnp.concatenate([carry_ref[:, r, :] for r in range(share)], axis=0)
    state_b = jnp.concatenate([carry_ref[:, share + r, :] for r in range(share)], axis=0)
    for b in range(chunks):
        before = state_f
        mine_ref[b, :, 0:LANES] = (
            before * jnp.exp(half_ref[2 * b : 2 * b + 1, :])
        ).astype(BF16)
        state_f = state_f * decay_of(b, 0) + upd_ref[2 * b]
    for b in reversed(range(chunks)):
        mine_ref[b, :, LANES : 2 * LANES] = (
            state_b * jnp.exp(half_ref[2 * b + 1 : 2 * b + 2, :])
        ).astype(BF16)
        state_b = state_b * decay_of(b, 1) + upd_ref[2 * b + 1]

    def mix_copy(i):
        peer = lax.rem(row + i, members)
        return pltpu.make_async_remote_copy(
            src_ref=ks_ref.at[peer],
            dst_ref=mixed_ref.at[row],
            send_sem=mix_send_sem.at[i],
            recv_sem=mix_recv_sem.at[i],
            device_id={"tp": peer},
            device_id_type=MESH,
        )

    for b in range(chunks):
        rows = slice(b * CHUNK, (b + 1) * CHUNK)
        across = lax.dot_general(qs_ref[b], mine_ref[b], NT, preferred_element_type=F32)
        for h in range(2):
            o = out_ref[h, rows, :] + across[h * CHUNK : (h + 1) * CHUNK]
            cols = slice(h * DV, (h + 1) * DV)
            o = o * lax.rsqrt(jnp.mean(o * o, axis=-1, keepdims=True) + EPS)
            g = g_ref[rows, cols].astype(F32)
            o = o * gain_ref[0:1, cols] * (g / (1.0 + jnp.exp(-g)))
            ks_ref[b, :, cols] = o.astype(BF16)
    for i in range(1, members):
        mix_copy(i).start()
    mixed_ref[row] = ks_ref[row]
    for i in range(1, members):
        mix_copy(i).wait()


def attention(mesh, queries, key_rows, values, out_gate, fwd_decay, bwd_decay, head_gain):
    groups, members = mesh.shape["sp"], mesh.shape["tp"]
    span = queries.shape[0]
    chunks = span // CHUNK
    share = DV // groups
    inner, outer = rope_tables(span, groups)
    vmem = pl.BlockSpec(memory_space=pltpu.VMEM)
    outer_row = lax.dynamic_index_in_dim(
        jnp.asarray(outer), lax.axis_index("sp"), 0, keepdims=False
    )
    return pl.pallas_call(
        functools.partial(attention_kernel, groups, members),
        out_shape=jax.ShapeDtypeStruct((members, CHUNK, 2 * DV), BF16),
        in_specs=[vmem] * 9,
        out_specs=vmem,
        scratch_shapes=[
            pltpu.VMEM((chunks, 2 * CHUNK, 2 * LANES), BF16),
            pltpu.VMEM((chunks, CHUNK, 2 * LANES), BF16),
            pltpu.VMEM((2, span, DV), F32),
            pltpu.VMEM((2 * chunks, DV, LANES), F32),
            pltpu.VMEM((2 * chunks, LANES), F32),
            pltpu.VMEM((groups * 4 * share, LANES), F32),
            pltpu.VMEM((groups * 4 * share, LANES), F32),
            pltpu.VMEM((groups, 2 * share, LANES), F32),
            pltpu.VMEM((groups, 2 * share, LANES), F32),
            pltpu.VMEM((chunks, DV, 2 * LANES), BF16),
            pltpu.SemaphoreType.DMA((groups,)),
            pltpu.SemaphoreType.DMA((groups,)),
            pltpu.SemaphoreType.DMA((groups,)),
            pltpu.SemaphoreType.DMA((groups,)),
            pltpu.SemaphoreType.DMA((members,)),
            pltpu.SemaphoreType.DMA((members,)),
        ],
        compiler_params=pltpu.CompilerParams(collective_id=0, has_side_effects=True),
        cost_estimate=pl.CostEstimate(flops=10**10, bytes_accessed=10**8, transcendentals=0),
        name="attention",
    )(
        queries,
        key_rows,
        values,
        out_gate,
        fwd_decay,
        bwd_decay,
        head_gain.reshape(1, -1),
        jnp.asarray(inner),
        outer_row,
    )


def exchange_kernel(groups, src_ref, dst_ref, own_sem, send_sem, recv_sem):
    me = lax.axis_index("sp")
    barrier = pltpu.get_barrier_semaphore()

    def greet(i, c):
        pl.semaphore_signal(
            barrier, inc=1, device_id={"sp": lax.rem(me + i, groups)}, device_id_type=MESH
        )
        return c

    lax.fori_loop(1, groups, greet, 0)
    own = pltpu.make_async_copy(src_ref.at[me], dst_ref.at[me], own_sem)
    own.start()
    pl.semaphore_wait(barrier, groups - 1)

    def copy(i):
        half = lax.div(i + 1, 2)
        shift = jnp.where(lax.rem(i, 2) == 1, half, groups - half)
        peer = lax.rem(me + shift, groups)
        return pltpu.make_async_remote_copy(
            src_ref=src_ref.at[peer],
            dst_ref=dst_ref.at[me],
            send_sem=send_sem.at[shift],
            recv_sem=recv_sem.at[shift],
            device_id={"sp": peer},
            device_id_type=MESH,
        )

    def start(i, c):
        copy(i).start()
        return c

    def finish(i, c):
        copy(i).wait()
        return c

    lax.fori_loop(1, groups, start, 0)
    lax.fori_loop(1, groups, finish, 0)
    own.wait()


def exchange(mesh, array, number):
    groups = mesh.shape["sp"]
    anywhere = pl.BlockSpec(memory_space=pl.ANY)
    return pl.pallas_call(
        functools.partial(exchange_kernel, groups),
        out_shape=jax.ShapeDtypeStruct(array.shape, array.dtype),
        in_specs=[anywhere],
        out_specs=anywhere,
        scratch_shapes=[
            pltpu.SemaphoreType.DMA,
            pltpu.SemaphoreType.DMA((groups,)),
            pltpu.SemaphoreType.DMA((groups,)),
        ],
        compiler_params=pltpu.CompilerParams(collective_id=number, has_side_effects=True),
        cost_estimate=pl.CostEstimate(flops=10**10, bytes_accessed=10**8, transcendentals=0),
        name="exchange",
    )(array)


def normalize(tensor):
    return tensor * lax.rsqrt(jnp.mean(tensor * tensor, axis=-1, keepdims=True) + EPS)


def dot(a, b):
    return jnp.dot(a, b, preferred_element_type=F32)


def silu(x):
    return x / (1.0 + jnp.exp(-x))


def body(
    mesh,
    stream,
    queries,
    key_rows,
    values,
    out_gate,
    fwd_decay,
    bwd_decay,
    head_gain,
    out_proj,
    mix_gain,
    ffn_gain,
    moe_gain,
    routes,
    route_weight,
    expert_gate,
    expert_up,
    expert_down,
    shared_gate,
    shared_up,
    shared_down,
):
    tokens, width = stream.shape
    experts, members = mesh.shape["sp"], mesh.shape["tp"]
    slots = experts * CAP
    gate_all = lax.all_gather(expert_gate[0], "tp", axis=0, tiled=False)
    up_all = lax.all_gather(expert_up[0], "tp", axis=0, tiled=False)
    down_all = lax.all_gather(expert_down[0], "tp", axis=0, tiled=True)

    flat = routes.reshape(-1)
    named = (flat[:, None] == jnp.arange(experts, dtype=jnp.int32)[None, :]).astype(BF16)
    count = tokens * TOPK
    earlier = (
        jnp.arange(count, dtype=jnp.int32)[:, None] > jnp.arange(count, dtype=jnp.int32)[None, :]
    ).astype(BF16)
    slot = jnp.sum(dot(earlier, named) * named.astype(F32), axis=1).astype(jnp.int32)
    place = (flat * CAP + slot).reshape(tokens, TOPK)
    where = jnp.arange(slots, dtype=jnp.int32)
    hit = place[:, :, None] == where[None, None, :]
    put = jnp.any(hit, axis=1).astype(BF16)
    weigh = jnp.sum(jnp.where(hit, route_weight[:, :, None], 0.0), axis=1)
    weigh_high = weigh.astype(BF16)
    weigh_low = (weigh - weigh_high.astype(F32)).astype(BF16)

    mixed = attention(
        mesh, queries, key_rows, values, out_gate, fwd_decay, bwd_decay, head_gain
    )
    mixed, shared_gate, shared_up, shared_down = lax.optimization_barrier(
        (mixed, shared_gate, shared_up, shared_down)
    )
    sgate_all = lax.all_gather(shared_gate, "tp", axis=0, tiled=False)
    sup_all = lax.all_gather(shared_up, "tp", axis=0, tiled=False)
    sdown_all = lax.all_gather(shared_down, "tp", axis=0, tiled=True)
    projected = sum(
        dot(mixed[i], out_proj[i * 2 * DV : (i + 1) * 2 * DV]) for i in range(members)
    )
    residual = (stream.astype(F32) + normalize(projected) * mix_gain).astype(BF16)
    normed = (normalize(residual.astype(F32)) * ffn_gain).astype(BF16)
    filled = lax.dot_general(put, normed, TN, preferred_element_type=F32).astype(BF16)
    lines = CAP * width // LANES
    arrived = exchange(mesh, filled.reshape(experts, lines, LANES), 1).reshape(slots, width)
    hidden = jnp.concatenate(
        [
            (silu(dot(arrived, gate_all[i])) * dot(arrived, up_all[i])).astype(BF16)
            for i in range(members)
        ],
        axis=1,
    )
    answer = dot(hidden, down_all).astype(BF16)
    returned = exchange(mesh, answer.reshape(experts, lines, LANES), 2).reshape(slots, width)
    returned, normed = lax.optimization_barrier((returned, normed))
    shared_hidden = jnp.concatenate(
        [
            (silu(dot(normed, sgate_all[i])) * dot(normed, sup_all[i])).astype(BF16)
            for i in range(members)
        ],
        axis=1,
    )
    mixture = (
        dot(shared_hidden, sdown_all) + dot(weigh_high, returned) + dot(weigh_low, returned)
    )
    return (residual.astype(F32) + normalize(mixture) * moe_gain).astype(BF16)


def solution(mesh):
    placed = (
        P(("sp", "tp"), None),
        P("sp", "tp"),
        P("sp", "tp"),
        P("sp", "tp"),
        P("sp", "tp"),
        P("sp", "tp"),
        P("sp", "tp"),
        P("tp"),
        P(),
        P(),
        P(),
        P(),
        P(("sp", "tp"), None),
        P(("sp", "tp"), None),
        P("sp", None, "tp"),
        P("sp", None, "tp"),
        P("sp", "tp", None),
        P(None, "tp"),
        P(None, "tp"),
        P("tp", None),
    )
    return jax.shard_map(
        functools.partial(body, mesh),
        mesh=mesh,
        in_specs=placed,
        out_specs=P(("sp", "tp"), None),
        check_vma=False,
    )
```

```python
import functools

import jax
import jax.numpy as jnp
import numpy as np
from jax import lax
from jax.experimental import pallas as pl
from jax.experimental.pallas import tpu as pltpu
from jax.sharding import PartitionSpec as P

KEY_CHANNELS = 64
DV = 128
TOPK = 2
CAP = 6
CHUNK = 128
LANES = 128
EPS = 1e-06
GATE_NORM = 16.0
ROPE_BASE = 10000.0
MESH = pl.DeviceIdType.MESH
NT = (((1,), (1,)), ((), ()))
TN = (((0,), (0,)), ((), ()))
F32 = jnp.float32
BF16 = jnp.bfloat16


def rope_tables(span, devices):
    half = KEY_CHANNELS // 2
    freq = ROPE_BASE ** (-np.arange(half, dtype=np.float64) / half)
    freq = np.tile(freq, LANES // half)
    inner = np.arange(span)[:, None] * freq[None, :]
    outer = (np.arange(devices) * span)[:, None] * freq[None, :]
    inner = np.stack([np.cos(inner), np.sin(inner)]).astype(np.float32)
    outer = np.stack([np.cos(outer), np.sin(outer)], axis=1).astype(np.float32)
    return inner, outer


def attention_kernel(
    groups,
    members,
    q_ref,
    k_ref,
    v_ref,
    g_ref,
    fd_ref,
    bd_ref,
    gain_ref,
    inner_ref,
    outer_ref,
    stream_ref,
    proj_hbm,
    mix_gain_ref,
    ffn_gain_ref,
    routes_ref,
    spread_ref,
    target_ref,
    gate_hbm,
    up_hbm,
    down_hbm,
    arrived_ref,
    residual_ref,
    normed_ref,
    put_ref,
    gate_all,
    up_all,
    down_all,
    mixed_ref,
    proj_ref,
    projected_ref,
    stage_ref,
    filled_ref,
    qs_ref,
    ks_ref,
    out_ref,
    upd_ref,
    half_ref,
    send_ref,
    got_ref,
    back_ref,
    carry_ref,
    mine_ref,
    send_sem,
    recv_sem,
    back_send_sem,
    back_recv_sem,
    mix_send_sem,
    mix_recv_sem,
    row_send_sem,
    row_recv_sem,
    near_send_sem,
    near_recv_sem,
    far_send_sem,
    far_recv_sem,
    local_sem,
):
    me = lax.axis_index("sp")
    row = lax.axis_index("tp")
    shards = (gate_hbm, up_hbm, down_hbm)
    wholes = (gate_all, up_all, down_all)
    sides = (lax.rem(row + 1, members), lax.rem(row + members - 1, members))
    proj_copy = pltpu.make_async_copy(proj_hbm, proj_ref, local_sem.at[0])
    proj_copy.start()
    own_copies = [
        pltpu.make_async_copy(shards[t], wholes[t].at[3], local_sem.at[1 + t]) for t in range(3)
    ]
    for copy in own_copies:
        copy.start()

    def near_copy(t, side):
        return pltpu.make_async_remote_copy(
            src_ref=shards[t],
            dst_ref=wholes[t].at[side],
            send_sem=near_send_sem.at[2 * t + side],
            recv_sem=near_recv_sem.at[2 * t + side],
            device_id={"tp": sides[side]},
            device_id_type=MESH,
        )

    def far_copy(t, side):
        half = shards[t].shape[0] // 2
        part = pl.ds(side * half, half)
        return pltpu.make_async_remote_copy(
            src_ref=wholes[t].at[side, part],
            dst_ref=wholes[t].at[2, part],
            send_sem=far_send_sem.at[2 * t + side],
            recv_sem=far_recv_sem.at[2 * t + side],
            device_id={"tp": sides[side]},
            device_id_type=MESH,
        )

    def send_near(t):
        for side in range(2):
            near_copy(t, side).start()

    def send_far(t):
        for side in range(2):
            near_copy(t, side).wait_recv()
            far_copy(t, side).start()

    span = q_ref.shape[0]
    chunks = span // CHUNK
    share = DV // groups
    message = 4 * share

    barrier = pltpu.get_barrier_semaphore()

    def greet(i, c):
        pl.semaphore_signal(
            barrier, inc=1, device_id={"sp": lax.rem(me + i, groups)}, device_id_type=MESH
        )
        return c

    lax.fori_loop(1, groups, greet, 0)
    for i in range(1, members):
        pl.semaphore_signal(
            barrier, inc=1, device_id={"tp": lax.rem(row + i, members)}, device_id_type=MESH
        )

    lane = lax.broadcasted_iota(jnp.int32, (CHUNK, LANES), 1)
    r_id = lax.broadcasted_iota(jnp.int32, (CHUNK, CHUNK), 0)
    c_id = lax.broadcasted_iota(jnp.int32, (CHUNK, CHUNK), 1)
    lower = r_id >= c_id
    upper = r_id <= c_id
    lower_one = jnp.where(lower, 1.0, 0.0).astype(BF16)
    upper_one = jnp.where(upper, 1.0, 0.0).astype(BF16)
    front = (lane % KEY_CHANNELS) < (KEY_CHANNELS // 2)
    first_head = lane < KEY_CHANNELS
    cos_0 = outer_ref[0:1, :]
    sin_0 = outer_ref[1:2, :]

    def log_decay(x):
        return (jnp.minimum(x, 0.0) - jnp.log1p(jnp.exp(-jnp.abs(x)))) * (1.0 / GATE_NORM)

    def cumulate(tri, x):
        high = x.astype(BF16)
        low = (x - high.astype(F32)).astype(BF16)
        return jnp.dot(tri, high, preferred_element_type=F32) + jnp.dot(
            tri, low, preferred_element_type=F32
        )

    for b in range(chunks):
        rows = slice(b * CHUNK, (b + 1) * CHUNK)
        cos_i = inner_ref[0, rows, :]
        sin_i = inner_ref[1, rows, :]
        cosine = cos_0 * cos_i - sin_0 * sin_i
        sine = sin_0 * cos_i + cos_0 * sin_i
        sine = jnp.where(front, -sine, sine)

        def rotated(u):
            swapped = jnp.where(
                front,
                pltpu.roll(u, LANES - KEY_CHANNELS // 2, 1),
                pltpu.roll(u, KEY_CHANNELS // 2, 1),
            )
            return u * cosine + swapped * sine

        q = rotated(q_ref[rows, :].astype(F32) * KEY_CHANNELS ** (-0.5))
        k = rotated(k_ref[rows, :].astype(F32))
        cf = cumulate(lower_one, log_decay(fd_ref[rows, :]))
        cb = cumulate(upper_one, log_decay(bd_ref[rows, :]))
        hf = cf[CHUNK - 1 : CHUNK, :] * 0.5
        hb = cb[0:1, :] * 0.5
        half_ref[2 * b : 2 * b + 1, :] = hf
        half_ref[2 * b + 1 : 2 * b + 2, :] = hb
        qf = q * jnp.exp(cf - hf)
        qb = q * jnp.exp(cb - hb)
        kf = (k * jnp.exp(hf - cf)).astype(BF16)
        kb = (k * jnp.exp(hb - cb)).astype(BF16)
        ks_ref[b, :, 0:LANES] = kf
        ks_ref[b, :, LANES : 2 * LANES] = kb
        qs_ref[b, 0:CHUNK, 0:LANES] = jnp.where(first_head, qf, 0.0).astype(BF16)
        qs_ref[b, 0:CHUNK, LANES : 2 * LANES] = jnp.where(first_head, qb, 0.0).astype(BF16)
        qs_ref[b, CHUNK : 2 * CHUNK, 0:LANES] = jnp.where(first_head, 0.0, qf).astype(BF16)
        qs_ref[b, CHUNK : 2 * CHUNK, LANES : 2 * LANES] = jnp.where(first_head, 0.0, qb).astype(
            BF16
        )
        both = lax.dot_general(
            v_ref[rows, :], ks_ref[b], TN, preferred_element_type=F32
        )
        upd_ref[2 * b] = jnp.where(
            first_head, both[0:DV, 0:LANES], both[DV : 2 * DV, 0:LANES]
        ) * jnp.exp(hf)
        upd_ref[2 * b + 1] = jnp.where(
            first_head, both[0:DV, LANES : 2 * LANES], both[DV : 2 * DV, LANES : 2 * LANES]
        ) * jnp.exp(hb)
        if b == 0:
            pl.semaphore_wait(barrier, groups - 1 + members - 1)
            send_near(0)

    def decay_of(b, d):
        return jnp.exp(half_ref[2 * b + d : 2 * b + d + 1, :] * 2.0)

    total_f = upd_ref[0]
    decay_f = decay_of(0, 0)
    for b in range(1, chunks):
        total_f = total_f * decay_of(b, 0) + upd_ref[2 * b]
        decay_f = decay_f * decay_of(b, 0)
    total_b = upd_ref[2 * (chunks - 1) + 1]
    decay_b = decay_of(chunks - 1, 1)
    for b in reversed(range(chunks - 1)):
        total_b = total_b * decay_of(b, 1) + upd_ref[2 * b + 1]
        decay_b = decay_b * decay_of(b, 1)
    for r in range(share):
        part = slice(r * groups, (r + 1) * groups)
        send_ref[pl.ds(r, groups, stride=message), :] = total_f[part, :]
        send_ref[pl.ds(share + r, groups, stride=message), :] = total_b[part, :]
        send_ref[pl.ds(2 * share + r, groups, stride=message), :] = jnp.broadcast_to(
            decay_f, (groups, LANES)
        )
        send_ref[pl.ds(3 * share + r, groups, stride=message), :] = jnp.broadcast_to(
            decay_b, (groups, LANES)
        )

    def block(ref, i):
        return ref.at[pl.ds(pl.multiple_of(i * message, message), message)]

    def half_block(ref, i):
        return ref.at[i]

    def out_copy(peer, i):
        return pltpu.make_async_remote_copy(
            src_ref=block(send_ref, peer),
            dst_ref=block(got_ref, me),
            send_sem=send_sem.at[i],
            recv_sem=recv_sem.at[i],
            device_id={"sp": peer},
            device_id_type=MESH,
        )

    def back_copy(peer, i):
        return pltpu.make_async_remote_copy(
            src_ref=half_block(back_ref, peer),
            dst_ref=half_block(carry_ref, me),
            send_sem=back_send_sem.at[i],
            recv_sem=back_recv_sem.at[i],
            device_id={"sp": peer},
            device_id_type=MESH,
        )

    def offset(i):
        half = lax.div(i + 1, 2)
        return jnp.where(lax.rem(i, 2) == 1, half, groups - half)

    def peer_of(i):
        return lax.rem(me + offset(i), groups)

    def each(action):
        def step(i, c):
            action(i)
            return c

        lax.fori_loop(1, groups, step, 0)

    each(lambda i: out_copy(peer_of(i), offset(i)).start())
    mine = pl.ds(pl.multiple_of(me * message, message), message)
    got_ref[mine, :] = send_ref[mine, :]

    for b in range(chunks):
        rows = slice(b * CHUNK, (b + 1) * CHUNK)
        s_f = lax.dot_general(
            qs_ref[b, :, 0:LANES], ks_ref[b, :, 0:LANES], NT, preferred_element_type=F32
        )
        s_b = lax.dot_general(
            qs_ref[b, :, LANES : 2 * LANES],
            ks_ref[b, :, LANES : 2 * LANES],
            NT,
            preferred_element_type=F32,
        )
        for h in range(2):
            part = slice(h * CHUNK, (h + 1) * CHUNK)
            s = jnp.where(lower, s_f[part], 0.0) + jnp.where(upper, s_b[part], 0.0)
            out_ref[h, rows, :] = jnp.dot(
                s.astype(BF16), v_ref[rows, h * DV : (h + 1) * DV], preferred_element_type=F32
            )

    each(lambda i: out_copy(peer_of(i), offset(i)).wait())

    zero = jnp.zeros((share, LANES), F32)

    def scan(s, carried):
        c_f, c_b = carried
        t = groups - 1 - s
        at_s = pl.multiple_of(s * message, message)
        at_t = pl.multiple_of(t * message, message)
        m_s = got_ref[pl.ds(at_s, message), :]
        m_t = got_ref[pl.ds(at_t, message), :]
        back_ref[s, 0:share, :] = c_f
        back_ref[t, share : 2 * share, :] = c_b
        c_f = c_f * m_s[2 * share : 3 * share] + m_s[0:share]
        c_b = c_b * m_t[3 * share : 4 * share] + m_t[share : 2 * share]
        return c_f, c_b

    lax.fori_loop(0, groups, scan, (zero, zero))
    each(lambda i: back_copy(peer_of(i), offset(i)).start())
    carry_ref[me] = back_ref[me]
    send_far(0)
    each(lambda i: back_copy(peer_of(i), offset(i)).wait())

    state_f = jnp.concatenate([carry_ref[:, r, :] for r in range(share)], axis=0)
    state_b = jnp.concatenate([carry_ref[:, share + r, :] for r in range(share)], axis=0)
    for b in range(chunks):
        before = state_f
        mine_ref[b, :, 0:LANES] = (
            before * jnp.exp(half_ref[2 * b : 2 * b + 1, :])
        ).astype(BF16)
        state_f = state_f * decay_of(b, 0) + upd_ref[2 * b]
    for b in reversed(range(chunks)):
        mine_ref[b, :, LANES : 2 * LANES] = (
            state_b * jnp.exp(half_ref[2 * b + 1 : 2 * b + 2, :])
        ).astype(BF16)
        state_b = state_b * decay_of(b, 1) + upd_ref[2 * b + 1]

    def mix_copy(i):
        peer = lax.rem(row + i, members)
        return pltpu.make_async_remote_copy(
            src_ref=ks_ref.at[peer],
            dst_ref=mixed_ref.at[row],
            send_sem=mix_send_sem.at[i],
            recv_sem=mix_recv_sem.at[i],
            device_id={"tp": peer},
            device_id_type=MESH,
        )

    for b in range(chunks):
        rows = slice(b * CHUNK, (b + 1) * CHUNK)
        across = lax.dot_general(qs_ref[b], mine_ref[b], NT, preferred_element_type=F32)
        for h in range(2):
            o = out_ref[h, rows, :] + across[h * CHUNK : (h + 1) * CHUNK]
            cols = slice(h * DV, (h + 1) * DV)
            o = o * lax.rsqrt(jnp.mean(o * o, axis=-1, keepdims=True) + EPS)
            g = g_ref[rows, cols].astype(F32)
            o = o * gain_ref[0:1, cols] * (g / (1.0 + jnp.exp(-g)))
            ks_ref[b, :, cols] = o.astype(BF16)
    for i in range(1, members):
        mix_copy(i).start()
    send_near(1)
    send_near(2)
    mixed_ref[row] = ks_ref[row]

    count = normed_ref.shape[0]
    width = normed_ref.shape[1]
    lines = width // LANES
    expert_id = lax.broadcasted_iota(jnp.int32, (count, LANES), 1)
    token_id = lax.broadcasted_iota(jnp.int32, (count, count), 0)
    other_id = lax.broadcasted_iota(jnp.int32, (count, count), 1)
    named = jnp.where(routes_ref[:, 0:1] == expert_id, 1.0, 0.0) + jnp.where(
        routes_ref[:, 1:2] == expert_id, 1.0, 0.0
    )
    earlier = jnp.where(token_id > other_id, 1.0, 0.0).astype(BF16)
    rank = jnp.dot(earlier, named.astype(BF16), preferred_element_type=F32)
    ranked = (named * (rank + 1.0)).astype(BF16)
    spread = jnp.dot(ranked, spread_ref[...], preferred_element_type=F32)
    put_ref[...] = jnp.where(spread == target_ref[...], 1.0, 0.0).astype(BF16)

    proj_copy.wait()
    for i in range(1, members):
        mix_copy(i).wait()
    mixed = jnp.concatenate([mixed_ref[i] for i in range(members)], axis=1)
    step = min(512, width)
    for n in range(width // step):
        cols = slice(n * step, (n + 1) * step)
        projected_ref[:, cols] = jnp.dot(mixed, proj_ref[:, cols], preferred_element_type=F32)
    for i in range(count // 16):
        rows = slice(i * 16, (i + 1) * 16)
        p = projected_ref[rows, :]
        p = p * lax.rsqrt(jnp.mean(p * p, axis=-1, keepdims=True) + EPS) * mix_gain_ref[...]
        r = (stream_ref[rows, :].astype(F32) + p).astype(BF16)
        residual_ref[rows, :] = r
        r = r.astype(F32)
        r = r * lax.rsqrt(jnp.mean(r * r, axis=-1, keepdims=True) + EPS) * ffn_gain_ref[...]
        normed_ref[rows, :] = r.astype(BF16)
    slots = put_ref.shape[1]
    for n in range(width // (2 * LANES)):
        f = lax.dot_general(
            put_ref[...],
            normed_ref[:, n * 2 * LANES : (n + 1) * 2 * LANES],
            TN,
            preferred_element_type=F32,
        )
        stage_ref[pl.ds(2 * n, slots, stride=lines), :] = f[:, 0:LANES]
        stage_ref[pl.ds(2 * n + 1, slots, stride=lines), :] = f[:, LANES : 2 * LANES]
    piece = slots * lines // groups

    def narrow(i, c):
        rows = pl.ds(pl.multiple_of(i * piece, 16), piece)
        filled_ref[rows, :] = stage_ref[rows, :].astype(BF16)
        return c

    lax.fori_loop(0, groups, narrow, 0)

    def row_copy(peer, i):
        return pltpu.make_async_remote_copy(
            src_ref=filled_ref.at[pl.ds(pl.multiple_of(peer * piece, 16), piece)],
            dst_ref=arrived_ref.at[pl.ds(pl.multiple_of(me * piece, 16), piece)],
            send_sem=row_send_sem.at[i],
            recv_sem=row_recv_sem.at[i],
            device_id={"sp": peer},
            device_id_type=MESH,
        )

    each(lambda i: row_copy(peer_of(i), offset(i)).start())
    own = pl.ds(pl.multiple_of(me * piece, 16), piece)
    own_rows = pltpu.make_async_copy(filled_ref.at[own], arrived_ref.at[own], local_sem.at[4])
    own_rows.start()
    send_far(1)
    send_far(2)
    each(lambda i: row_copy(peer_of(i), offset(i)).wait())
    for t in range(3):
        for side in range(2):
            near_copy(t, side).wait_send()
            far_copy(t, side).wait()
    for copy in own_copies:
        copy.wait()
    own_rows.wait()


def attention(
    mesh,
    stream,
    queries,
    key_rows,
    values,
    out_gate,
    fwd_decay,
    bwd_decay,
    head_gain,
    out_proj,
    mix_gain,
    ffn_gain,
    routes,
    gate,
    up,
    down,
):
    groups, members = mesh.shape["sp"], mesh.shape["tp"]
    span = queries.shape[0]
    chunks = span // CHUNK
    share = DV // groups
    tokens, width = stream.shape
    slots = groups * CAP
    lines = width // LANES
    inner, outer = rope_tables(span, groups)
    vmem = pl.BlockSpec(memory_space=pltpu.VMEM)
    anywhere = pl.BlockSpec(memory_space=pl.ANY)
    outer_row = lax.dynamic_index_in_dim(
        jnp.asarray(outer), lax.axis_index("sp"), 0, keepdims=False
    )
    spread, target = slot_tables(groups)
    dma = pltpu.SemaphoreType.DMA
    return pl.pallas_call(
        functools.partial(attention_kernel, groups, members),
        out_shape=(
            jax.ShapeDtypeStruct((slots * lines, LANES), BF16),
            jax.ShapeDtypeStruct((tokens, width), BF16),
            jax.ShapeDtypeStruct((tokens, width), BF16),
            jax.ShapeDtypeStruct((tokens, slots), BF16),
            jax.ShapeDtypeStruct((4, *gate.shape), BF16),
            jax.ShapeDtypeStruct((4, *up.shape), BF16),
            jax.ShapeDtypeStruct((4, *down.shape), BF16),
        ),
        in_specs=[vmem] * 10 + [anywhere] + [vmem] * 5 + [anywhere] * 3,
        out_specs=(anywhere, vmem, vmem, vmem, anywhere, anywhere, anywhere),
        scratch_shapes=[
            pltpu.VMEM((members, CHUNK, 2 * DV), BF16),
            pltpu.VMEM(out_proj.shape, BF16),
            pltpu.VMEM((tokens, width), F32),
            pltpu.VMEM((slots * lines, LANES), F32),
            pltpu.VMEM((slots * lines, LANES), BF16),
            pltpu.VMEM((chunks, 2 * CHUNK, 2 * LANES), BF16),
            pltpu.VMEM((chunks, CHUNK, 2 * LANES), BF16),
            pltpu.VMEM((2, span, DV), F32),
            pltpu.VMEM((2 * chunks, DV, LANES), F32),
            pltpu.VMEM((2 * chunks, LANES), F32),
            pltpu.VMEM((groups * 4 * share, LANES), F32),
            pltpu.VMEM((groups * 4 * share, LANES), F32),
            pltpu.VMEM((groups, 2 * share, LANES), F32),
            pltpu.VMEM((groups, 2 * share, LANES), F32),
            pltpu.VMEM((chunks, DV, 2 * LANES), BF16),
            dma((groups,)),
            dma((groups,)),
            dma((groups,)),
            dma((groups,)),
            dma((members,)),
            dma((members,)),
            dma((groups,)),
            dma((groups,)),
            dma((6,)),
            dma((6,)),
            dma((6,)),
            dma((6,)),
            dma((5,)),
        ],
        compiler_params=pltpu.CompilerParams(collective_id=0, has_side_effects=True),
        cost_estimate=pl.CostEstimate(flops=10**10, bytes_accessed=10**8, transcendentals=0),
        name="attention",
    )(
        queries,
        key_rows,
        values,
        out_gate,
        fwd_decay,
        bwd_decay,
        head_gain.reshape(1, -1),
        jnp.asarray(inner),
        outer_row,
        stream,
        out_proj,
        mix_gain.reshape(1, -1),
        ffn_gain.reshape(1, -1),
        routes,
        jnp.asarray(spread).astype(BF16),
        jnp.asarray(target),
        gate,
        up,
        down,
    )


def slot_tables(experts):
    slot = np.arange(experts * CAP)
    spread = (np.arange(LANES)[:, None] == slot[None, :] // CAP).astype(np.float32)
    target = (slot % CAP + 1).astype(np.float32).reshape(1, -1)
    return spread, target


def experts_kernel(x_ref, gate_ref, up_ref, down_ref, out_ref, acc_ref):
    q = pl.program_id(0)
    x = x_ref[...]
    g = jnp.dot(x, gate_ref[0], preferred_element_type=F32)
    u = jnp.dot(x, up_ref[0], preferred_element_type=F32)
    h = (g / (1.0 + jnp.exp(-g)) * u).astype(BF16)
    width = out_ref.shape[1]
    step = min(512, width)
    for n in range(width // step):
        cols = slice(n * step, (n + 1) * step)
        part = jnp.dot(h, down_ref[0, :, cols], preferred_element_type=F32)

        @pl.when(q == 0)
        def _():
            acc_ref[:, cols] = part

        @pl.when(q > 0)
        def _():
            acc_ref[:, cols] += part

    @pl.when(q == pl.num_programs(0) - 1)
    def _():
        out_ref[...] = acc_ref[...].astype(BF16)


def expert_rows(x, gate, up, down):
    number = gate.shape[0]
    whole = pl.BlockSpec(x.shape, lambda q: (0, 0))
    return pl.pallas_call(
        experts_kernel,
        out_shape=jax.ShapeDtypeStruct(x.shape, BF16),
        grid=(number,),
        in_specs=[
            whole,
            pl.BlockSpec((1, *gate.shape[1:]), lambda q: (q, 0, 0)),
            pl.BlockSpec((1, *up.shape[1:]), lambda q: (q, 0, 0)),
            pl.BlockSpec((1, *down.shape[1:]), lambda q: (q, 0, 0)),
        ],
        out_specs=whole,
        scratch_shapes=[pltpu.VMEM(x.shape, F32)],
        name="experts",
    )(x, gate, up, down)


def return_kernel(
    groups,
    members,
    answer_ref,
    normed_ref,
    residual_ref,
    put_ref,
    routes_ref,
    weight_ref,
    spread_ref,
    moe_gain_ref,
    gate_ref,
    up_ref,
    down_ref,
    out_ref,
    back_ref,
    stage_ref,
    rows_ref,
    total_ref,
    gate_all,
    up_all,
    down_all,
    row_send_sem,
    row_recv_sem,
    near_send_sem,
    near_recv_sem,
    far_send_sem,
    far_recv_sem,
    twin_send_sem,
    twin_recv_sem,
    local_sem,
):
    me = lax.axis_index("sp")
    row = lax.axis_index("tp")
    core = lax.rem(me, 2)
    twin = me + 1 - 2 * core
    sides = (lax.rem(row + 1, members), lax.rem(row + members - 1, members))
    shards = (gate_ref, up_ref, down_ref)
    wholes = (gate_all, up_all, down_all)
    barrier = pltpu.get_barrier_semaphore()

    def greet(i, c):
        pl.semaphore_signal(
            barrier, inc=1, device_id={"sp": lax.rem(me + i, groups)}, device_id_type=MESH
        )
        return c

    lax.fori_loop(1, groups, greet, 0)
    for side in range(2):
        pl.semaphore_signal(barrier, inc=1, device_id={"tp": sides[side]}, device_id_type=MESH)
    slots = put_ref.shape[1]
    count, width = normed_ref.shape
    lines = width // LANES
    piece = slots * lines // groups
    own = pl.ds(pl.multiple_of(me * piece, 16), piece)
    own_rows = pltpu.make_async_copy(answer_ref.at[own], back_ref.at[own], local_sem.at[0])
    own_rows.start()
    pl.semaphore_wait(barrier, groups - 1 + 2)

    def offset(i):
        half = lax.div(i + 1, 2)
        return jnp.where(lax.rem(i, 2) == 1, half, groups - half)

    def row_copy(i):
        peer = lax.rem(me + offset(i), groups)
        return pltpu.make_async_remote_copy(
            src_ref=answer_ref.at[pl.ds(pl.multiple_of(peer * piece, 16), piece)],
            dst_ref=back_ref.at[own],
            send_sem=row_send_sem.at[offset(i)],
            recv_sem=row_recv_sem.at[offset(i)],
            device_id={"sp": peer},
            device_id_type=MESH,
        )

    def each(action):
        def step(i, c):
            action(i)
            return c

        lax.fori_loop(1, groups, step, 0)

    each(lambda i: row_copy(i).start())

    def half_of(t):
        h = shards[t].shape[0] // 2
        return pl.ds(pl.multiple_of(core * h, 16), h)

    def quarter_of(t, side):
        h = shards[t].shape[0] // 2
        return pl.ds(pl.multiple_of(core * h + side * (h // 2), 16), h // 2)

    def near_copy(t, side):
        return pltpu.make_async_remote_copy(
            src_ref=shards[t].at[half_of(t)],
            dst_ref=wholes[t].at[side, half_of(t)],
            send_sem=near_send_sem.at[2 * t + side],
            recv_sem=near_recv_sem.at[2 * t + side],
            device_id={"tp": sides[side]},
            device_id_type=MESH,
        )

    def far_copy(t, side):
        return pltpu.make_async_remote_copy(
            src_ref=wholes[t].at[side, quarter_of(t, side)],
            dst_ref=wholes[t].at[2, quarter_of(t, side)],
            send_sem=far_send_sem.at[2 * t + side],
            recv_sem=far_recv_sem.at[2 * t + side],
            device_id={"tp": sides[side]},
            device_id_type=MESH,
        )

    def twin_half(t):
        h = shards[t].shape[0] // 2
        return pl.ds(pl.multiple_of((1 - core) * h, 16), h)

    def twin_copy(t, k, part):
        return pltpu.make_async_remote_copy(
            src_ref=wholes[t].at[k, part],
            dst_ref=wholes[t].at[k, part],
            send_sem=twin_send_sem.at[3 * t + k],
            recv_sem=twin_recv_sem.at[3 * t + k],
            device_id={"sp": twin},
            device_id_type=MESH,
        )

    for t in range(3):
        for side in range(2):
            near_copy(t, side).start()

    expert_id = lax.broadcasted_iota(jnp.int32, (count, LANES), 1)
    weigh = jnp.where(routes_ref[:, 0:1] == expert_id, weight_ref[:, 0:1], 0.0) + jnp.where(
        routes_ref[:, 1:2] == expert_id, weight_ref[:, 1:2], 0.0
    )
    high = weigh.astype(BF16)
    low = (weigh - high.astype(F32)).astype(BF16)
    put = put_ref[...].astype(F32)
    high = (jnp.dot(high, spread_ref[...], preferred_element_type=F32) * put).astype(BF16)
    low = (jnp.dot(low, spread_ref[...], preferred_element_type=F32) * put).astype(BF16)

    step = min(512, width)

    def shared(gate, up, down, first):
        x = normed_ref[...]
        g = jnp.dot(x, gate[...], preferred_element_type=F32)
        u = jnp.dot(x, up[...], preferred_element_type=F32)
        h = (g / (1.0 + jnp.exp(-g)) * u).astype(BF16)
        for n in range(width // step):
            cols = slice(n * step, (n + 1) * step)
            part = jnp.dot(h, down[:, cols], preferred_element_type=F32)
            if first:
                total_ref[:, cols] = part
            else:
                total_ref[:, cols] += part

    shared(gate_ref, up_ref, down_ref, True)
    for t in range(3):
        for side in range(2):
            near_copy(t, side).wait_recv()
            far_copy(t, side).start()
            twin_copy(t, side, half_of(t)).start()
    for t in range(3):
        for side in range(2):
            far_copy(t, side).wait_recv()
        twin_copy(t, 2, half_of(t)).start()
    for k in range(3):
        for t in range(3):
            twin_copy(t, k, twin_half(t)).wait_recv()
        shared(gate_all.at[k], up_all.at[k], down_all.at[k], False)
    for t in range(3):
        for side in range(2):
            near_copy(t, side).wait_send()
            far_copy(t, side).wait_send()
        for k in range(3):
            twin_copy(t, k, half_of(t)).wait_send()

    own_rows.wait()
    each(lambda i: row_copy(i).wait())

    def widen(i, c):
        rows = pl.ds(pl.multiple_of(i * piece, 16), piece)
        stage_ref[rows, :] = back_ref[rows, :].astype(F32)
        return c

    lax.fori_loop(0, groups, widen, 0)
    for n in range(lines):
        rows_ref[:, n * LANES : (n + 1) * LANES] = stage_ref[
            pl.ds(n, slots, stride=lines), :
        ].astype(BF16)
    for n in range(width // step):
        cols = slice(n * step, (n + 1) * step)
        total_ref[:, cols] += jnp.dot(
            high, rows_ref[:, cols], preferred_element_type=F32
        ) + jnp.dot(low, rows_ref[:, cols], preferred_element_type=F32)
    for i in range(count // 16):
        rows = slice(i * 16, (i + 1) * 16)
        m = total_ref[rows, :]
        m = m * lax.rsqrt(jnp.mean(m * m, axis=-1, keepdims=True) + EPS) * moe_gain_ref[...]
        out_ref[rows, :] = (residual_ref[rows, :].astype(F32) + m).astype(BF16)


def returned(
    mesh,
    answer,
    normed,
    residual,
    put,
    routes,
    route_weight,
    moe_gain,
    shared_gate,
    shared_up,
    shared_down,
):
    groups, members = mesh.shape["sp"], mesh.shape["tp"]
    tokens, width = normed.shape
    slots = groups * CAP
    spread, _ = slot_tables(groups)
    vmem = pl.BlockSpec(memory_space=pltpu.VMEM)
    anywhere = pl.BlockSpec(memory_space=pl.ANY)
    dma = pltpu.SemaphoreType.DMA
    return pl.pallas_call(
        functools.partial(return_kernel, groups, members),
        out_shape=jax.ShapeDtypeStruct((tokens, width), BF16),
        in_specs=[anywhere] + [vmem] * 10,
        out_specs=vmem,
        scratch_shapes=[
            pltpu.VMEM(answer.shape, BF16),
            pltpu.VMEM(answer.shape, F32),
            pltpu.VMEM((slots, width), BF16),
            pltpu.VMEM((tokens, width), F32),
            pltpu.VMEM((3, *shared_gate.shape), BF16),
            pltpu.VMEM((3, *shared_up.shape), BF16),
            pltpu.VMEM((3, *shared_down.shape), BF16),
            dma((groups,)),
            dma((groups,)),
            dma((6,)),
            dma((6,)),
            dma((6,)),
            dma((6,)),
            dma((9,)),
            dma((9,)),
            dma((1,)),
        ],
        compiler_params=pltpu.CompilerParams(collective_id=1, has_side_effects=True),
        cost_estimate=pl.CostEstimate(flops=10**10, bytes_accessed=10**8, transcendentals=0),
        name="returned",
    )(
        answer,
        normed,
        residual,
        put,
        routes,
        route_weight,
        jnp.asarray(spread).astype(BF16),
        moe_gain.reshape(1, -1),
        shared_gate,
        shared_up,
        shared_down,
    )


def body(
    mesh,
    stream,
    queries,
    key_rows,
    values,
    out_gate,
    fwd_decay,
    bwd_decay,
    head_gain,
    out_proj,
    mix_gain,
    ffn_gain,
    moe_gain,
    routes,
    route_weight,
    expert_gate,
    expert_up,
    expert_down,
    shared_gate,
    shared_up,
    shared_down,
):
    width = stream.shape[1]
    slots = mesh.shape["sp"] * CAP
    arrived, residual, normed, put, gate, up, down = attention(
        mesh,
        stream,
        queries,
        key_rows,
        values,
        out_gate,
        fwd_decay,
        bwd_decay,
        head_gain,
        out_proj,
        mix_gain,
        ffn_gain,
        routes,
        expert_gate[0],
        expert_up[0],
        expert_down[0],
    )
    answer = expert_rows(arrived.reshape(slots, width), gate, up, down)
    return returned(
        mesh,
        answer.reshape(slots * width // LANES, LANES),
        normed,
        residual,
        put,
        routes,
        route_weight,
        moe_gain,
        shared_gate,
        shared_up,
        shared_down,
    )


def solution(mesh):
    placed = (
        P(("sp", "tp"), None),
        P("sp", "tp"),
        P("sp", "tp"),
        P("sp", "tp"),
        P("sp", "tp"),
        P("sp", "tp"),
        P("sp", "tp"),
        P("tp"),
        P(),
        P(),
        P(),
        P(),
        P(("sp", "tp"), None),
        P(("sp", "tp"), None),
        P("sp", None, "tp"),
        P("sp", None, "tp"),
        P("sp", "tp", None),
        P(None, "tp"),
        P(None, "tp"),
        P("tp", None),
    )
    return jax.shard_map(
        functools.partial(body, mesh),
        mesh=mesh,
        in_specs=placed,
        out_specs=P(("sp", "tp"), None),
        check_vma=False,
    )
```

```python
import functools

import jax
import jax.numpy as jnp
import numpy as np
from jax import lax
from jax.experimental import pallas as pl
from jax.experimental.pallas import tpu as pltpu
from jax.sharding import PartitionSpec as P

KEY_CHANNELS = 64
DV = 128
TOPK = 2
CAP = 6
CHUNK = 128
LANES = 128
EPS = 1e-06
GATE_NORM = 16.0
ROPE_BASE = 10000.0
MESH = pl.DeviceIdType.MESH
NT = (((1,), (1,)), ((), ()))
TN = (((0,), (0,)), ((), ()))
F32 = jnp.float32
BF16 = jnp.bfloat16


def rope_tables(span, devices):
    half = KEY_CHANNELS // 2
    freq = ROPE_BASE ** (-np.arange(half, dtype=np.float64) / half)
    freq = np.tile(freq, LANES // half)
    inner = np.arange(span)[:, None] * freq[None, :]
    outer = (np.arange(devices) * span)[:, None] * freq[None, :]
    inner = np.stack([np.cos(inner), np.sin(inner)]).astype(np.float32)
    outer = np.stack([np.cos(outer), np.sin(outer)], axis=1).astype(np.float32)
    return inner, outer


def layer_kernel(
    groups,
    members,
    q_ref,
    k_ref,
    v_ref,
    g_ref,
    fd_ref,
    bd_ref,
    gain_ref,
    inner_ref,
    outer_ref,
    stream_ref,
    mix_gain_ref,
    ffn_gain_ref,
    moe_gain_ref,
    routes_ref,
    weight_ref,
    spread_ref,
    target_ref,
    sgate_ref,
    sup_ref,
    sdown_ref,
    proj_hbm,
    gate_hbm,
    up_hbm,
    down_hbm,
    updated_ref,
    proj_ref,
    gate_all,
    up_all,
    down_all,
    sgate_all,
    sup_all,
    sdown_all,
    mixed_ref,
    total_ref,
    residual_ref,
    normed_ref,
    put_ref,
    stage_ref,
    filled_ref,
    arrived_ref,
    back_ref,
    x_ref,
    hidden_ref,
    qs_ref,
    ks_ref,
    out_ref,
    upd_ref,
    half_ref,
    send_ref,
    got_ref,
    back_state_ref,
    carry_ref,
    mine_ref,
    send_sem,
    recv_sem,
    back_send_sem,
    back_recv_sem,
    mix_send_sem,
    mix_recv_sem,
    row_send_sem,
    row_recv_sem,
    near_send_sem,
    near_recv_sem,
    far_send_sem,
    far_recv_sem,
    twin_send_sem,
    twin_recv_sem,
    local_sem,
):
    me = lax.axis_index("sp")
    row = lax.axis_index("tp")
    core = lax.rem(me, 2)
    twin = me + 1 - 2 * core
    span = q_ref.shape[0]
    chunks = span // CHUNK
    share = DV // groups
    message = 4 * share
    count, width = stream_ref.shape
    lines = width // LANES
    slots = put_ref.shape[0]
    half_lines = lines // 2
    half_rows = slots * half_lines
    piece = half_rows // groups
    inner_width = gate_hbm.shape[1]
    sides = (lax.rem(row + 1, members), lax.rem(row + members - 1, members))

    barrier = pltpu.get_barrier_semaphore()

    def greet(i, c):
        pl.semaphore_signal(
            barrier, inc=1, device_id={"sp": lax.rem(me + i, groups)}, device_id_type=MESH
        )
        return c

    lax.fori_loop(1, groups, greet, 0)
    for i in range(1, members):
        pl.semaphore_signal(
            barrier, inc=1, device_id={"tp": lax.rem(row + i, members)}, device_id_type=MESH
        )

    own_down = pl.ds(0, inner_width)
    local_copies = [
        pltpu.make_async_copy(proj_hbm, proj_ref, local_sem.at[0]),
        pltpu.make_async_copy(gate_hbm, gate_all.at[0], local_sem.at[1]),
        pltpu.make_async_copy(up_hbm, up_all.at[0], local_sem.at[2]),
        pltpu.make_async_copy(down_hbm, down_all.at[own_down], local_sem.at[3]),
    ]
    for copy in local_copies:
        copy.start()

    half_width = width // 2

    def place(t, slot, start, size):
        if t < 2:
            whole = (gate_all, up_all)[t]
            return whole.at[slot, pl.ds(start, size)]
        cols = pl.ds((t - 2) * half_width, half_width)
        return down_all.at[pl.ds(slot * inner_width + start, size), cols]

    def shard(t):
        if t < 2:
            return (gate_hbm, up_hbm)[t]
        return down_hbm.at[:, pl.ds((t - 2) * half_width, half_width)]

    def depth(t):
        return width if t < 2 else inner_width

    def near_copy(t, side):
        return pltpu.make_async_remote_copy(
            src_ref=shard(t),
            dst_ref=place(t, 1 + side, 0, depth(t)),
            send_sem=near_send_sem.at[2 * t + side],
            recv_sem=near_recv_sem.at[2 * t + side],
            device_id={"tp": sides[side]},
            device_id_type=MESH,
        )

    def far_copy(t, side):
        h = depth(t) // 2
        return pltpu.make_async_remote_copy(
            src_ref=place(t, 1 + side, side * h, h),
            dst_ref=place(t, 3, side * h, h),
            send_sem=far_send_sem.at[2 * t + side],
            recv_sem=far_recv_sem.at[2 * t + side],
            device_id={"tp": sides[side]},
            device_id_type=MESH,
        )

    def send_near(t):
        for side in range(2):
            near_copy(t, side).start()

    def send_far(t):
        for side in range(2):
            near_copy(t, side).wait_recv()
            far_copy(t, side).start()

    shared_own = (sgate_ref, sup_ref, sdown_ref)
    shared_all = (sgate_all, sup_all, sdown_all)

    def half_of(t, who):
        h = shared_own[t].shape[0] // 2
        return pl.ds(pl.multiple_of(who * h, 16), h)

    def quarter_of(t, side):
        h = shared_own[t].shape[0] // 2
        return pl.ds(pl.multiple_of(core * h + side * (h // 2), 16), h // 2)

    def shared_near(t, side):
        return pltpu.make_async_remote_copy(
            src_ref=shared_own[t].at[half_of(t, core)],
            dst_ref=shared_all[t].at[side, half_of(t, core)],
            send_sem=near_send_sem.at[8 + 2 * t + side],
            recv_sem=near_recv_sem.at[8 + 2 * t + side],
            device_id={"tp": sides[side]},
            device_id_type=MESH,
        )

    def shared_far(t, side):
        return pltpu.make_async_remote_copy(
            src_ref=shared_all[t].at[side, quarter_of(t, side)],
            dst_ref=shared_all[t].at[2, quarter_of(t, side)],
            send_sem=far_send_sem.at[8 + 2 * t + side],
            recv_sem=far_recv_sem.at[8 + 2 * t + side],
            device_id={"tp": sides[side]},
            device_id_type=MESH,
        )

    def twin_copy(t, k, part):
        return pltpu.make_async_remote_copy(
            src_ref=shared_all[t].at[k, part],
            dst_ref=shared_all[t].at[k, part],
            send_sem=twin_send_sem.at[3 * t + k],
            recv_sem=twin_recv_sem.at[3 * t + k],
            device_id={"sp": twin},
            device_id_type=MESH,
        )

    lane = lax.broadcasted_iota(jnp.int32, (CHUNK, LANES), 1)
    r_id = lax.broadcasted_iota(jnp.int32, (CHUNK, CHUNK), 0)
    c_id = lax.broadcasted_iota(jnp.int32, (CHUNK, CHUNK), 1)
    lower = r_id >= c_id
    upper = r_id <= c_id
    lower_one = jnp.where(lower, 1.0, 0.0).astype(BF16)
    upper_one = jnp.where(upper, 1.0, 0.0).astype(BF16)
    front = (lane % KEY_CHANNELS) < (KEY_CHANNELS // 2)
    first_head = lane < KEY_CHANNELS
    cos_0 = outer_ref[me, 0:1, :]
    sin_0 = outer_ref[me, 1:2, :]

    def log_decay(x):
        return (jnp.minimum(x, 0.0) - jnp.log1p(jnp.exp(-jnp.abs(x)))) * (1.0 / GATE_NORM)

    def cumulate(tri, x):
        high = x.astype(BF16)
        low = (x - high.astype(F32)).astype(BF16)
        return jnp.dot(tri, high, preferred_element_type=F32) + jnp.dot(
            tri, low, preferred_element_type=F32
        )

    for b in range(chunks):
        rows = slice(b * CHUNK, (b + 1) * CHUNK)
        cos_i = inner_ref[0, rows, :]
        sin_i = inner_ref[1, rows, :]
        cosine = cos_0 * cos_i - sin_0 * sin_i
        sine = sin_0 * cos_i + cos_0 * sin_i
        sine = jnp.where(front, -sine, sine)

        def rotated(u):
            swapped = jnp.where(
                front,
                pltpu.roll(u, LANES - KEY_CHANNELS // 2, 1),
                pltpu.roll(u, KEY_CHANNELS // 2, 1),
            )
            return u * cosine + swapped * sine

        q = rotated(q_ref[rows, :].astype(F32) * KEY_CHANNELS ** (-0.5))
        k = rotated(k_ref[rows, :].astype(F32))
        cf = cumulate(lower_one, log_decay(fd_ref[rows, :]))
        cb = cumulate(upper_one, log_decay(bd_ref[rows, :]))
        hf = cf[CHUNK - 1 : CHUNK, :] * 0.5
        hb = cb[0:1, :] * 0.5
        half_ref[2 * b : 2 * b + 1, :] = hf
        half_ref[2 * b + 1 : 2 * b + 2, :] = hb
        qf = q * jnp.exp(cf - hf)
        qb = q * jnp.exp(cb - hb)
        kf = (k * jnp.exp(hf - cf)).astype(BF16)
        kb = (k * jnp.exp(hb - cb)).astype(BF16)
        ks_ref[b, :, 0:LANES] = kf
        ks_ref[b, :, LANES : 2 * LANES] = kb
        qs_ref[b, 0:CHUNK, 0:LANES] = jnp.where(first_head, qf, 0.0).astype(BF16)
        qs_ref[b, 0:CHUNK, LANES : 2 * LANES] = jnp.where(first_head, qb, 0.0).astype(BF16)
        qs_ref[b, CHUNK : 2 * CHUNK, 0:LANES] = jnp.where(first_head, 0.0, qf).astype(BF16)
        qs_ref[b, CHUNK : 2 * CHUNK, LANES : 2 * LANES] = jnp.where(first_head, 0.0, qb).astype(
            BF16
        )
        both = lax.dot_general(
            v_ref[rows, :], ks_ref[b], TN, preferred_element_type=F32
        )
        upd_ref[2 * b] = jnp.where(
            first_head, both[0:DV, 0:LANES], both[DV : 2 * DV, 0:LANES]
        ) * jnp.exp(hf)
        upd_ref[2 * b + 1] = jnp.where(
            first_head, both[0:DV, LANES : 2 * LANES], both[DV : 2 * DV, LANES : 2 * LANES]
        ) * jnp.exp(hb)
        if b == 0:
            pl.semaphore_wait(barrier, groups - 1 + members - 1)
            send_near(0)

    def decay_of(b, d):
        return jnp.exp(half_ref[2 * b + d : 2 * b + d + 1, :] * 2.0)

    total_f = upd_ref[0]
    decay_f = decay_of(0, 0)
    for b in range(1, chunks):
        total_f = total_f * decay_of(b, 0) + upd_ref[2 * b]
        decay_f = decay_f * decay_of(b, 0)
    total_b = upd_ref[2 * (chunks - 1) + 1]
    decay_b = decay_of(chunks - 1, 1)
    for b in reversed(range(chunks - 1)):
        total_b = total_b * decay_of(b, 1) + upd_ref[2 * b + 1]
        decay_b = decay_b * decay_of(b, 1)
    for r in range(share):
        part = slice(r * groups, (r + 1) * groups)
        send_ref[pl.ds(r, groups, stride=message), :] = total_f[part, :]
        send_ref[pl.ds(share + r, groups, stride=message), :] = total_b[part, :]
        send_ref[pl.ds(2 * share + r, groups, stride=message), :] = jnp.broadcast_to(
            decay_f, (groups, LANES)
        )
        send_ref[pl.ds(3 * share + r, groups, stride=message), :] = jnp.broadcast_to(
            decay_b, (groups, LANES)
        )

    def block(ref, i):
        return ref.at[pl.ds(pl.multiple_of(i * message, message), message)]

    def half_block(ref, i):
        return ref.at[i]

    def out_copy(peer, i):
        return pltpu.make_async_remote_copy(
            src_ref=block(send_ref, peer),
            dst_ref=block(got_ref, me),
            send_sem=send_sem.at[i],
            recv_sem=recv_sem.at[i],
            device_id={"sp": peer},
            device_id_type=MESH,
        )

    def back_copy(peer, i):
        return pltpu.make_async_remote_copy(
            src_ref=half_block(back_state_ref, peer),
            dst_ref=half_block(carry_ref, me),
            send_sem=back_send_sem.at[i],
            recv_sem=back_recv_sem.at[i],
            device_id={"sp": peer},
            device_id_type=MESH,
        )

    def offset(i):
        half = lax.div(i + 1, 2)
        return jnp.where(lax.rem(i, 2) == 1, half, groups - half)

    def peer_of(i):
        return lax.rem(me + offset(i), groups)

    def each(action):
        def step(i, c):
            action(i)
            return c

        lax.fori_loop(1, groups, step, 0)

    each(lambda i: out_copy(peer_of(i), offset(i)).start())
    mine = pl.ds(pl.multiple_of(me * message, message), message)
    got_ref[mine, :] = send_ref[mine, :]

    for b in range(chunks):
        rows = slice(b * CHUNK, (b + 1) * CHUNK)
        s_f = lax.dot_general(
            qs_ref[b, :, 0:LANES], ks_ref[b, :, 0:LANES], NT, preferred_element_type=F32
        )
        s_b = lax.dot_general(
            qs_ref[b, :, LANES : 2 * LANES],
            ks_ref[b, :, LANES : 2 * LANES],
            NT,
            preferred_element_type=F32,
        )
        for h in range(2):
            part = slice(h * CHUNK, (h + 1) * CHUNK)
            s = jnp.where(lower, s_f[part], 0.0) + jnp.where(upper, s_b[part], 0.0)
            out_ref[h, rows, :] = jnp.dot(
                s.astype(BF16), v_ref[rows, h * DV : (h + 1) * DV], preferred_element_type=F32
            )

    each(lambda i: out_copy(peer_of(i), offset(i)).wait())

    zero = jnp.zeros((share, LANES), F32)

    def scan(s, carried):
        c_f, c_b = carried
        t = groups - 1 - s
        at_s = pl.multiple_of(s * message, message)
        at_t = pl.multiple_of(t * message, message)
        m_s = got_ref[pl.ds(at_s, message), :]
        m_t = got_ref[pl.ds(at_t, message), :]
        back_state_ref[s, 0:share, :] = c_f
        back_state_ref[t, share : 2 * share, :] = c_b
        c_f = c_f * m_s[2 * share : 3 * share] + m_s[0:share]
        c_b = c_b * m_t[3 * share : 4 * share] + m_t[share : 2 * share]
        return c_f, c_b

    lax.fori_loop(0, groups, scan, (zero, zero))
    each(lambda i: back_copy(peer_of(i), offset(i)).start())
    carry_ref[me] = back_state_ref[me]
    send_far(0)
    each(lambda i: back_copy(peer_of(i), offset(i)).wait())

    state_f = jnp.concatenate([carry_ref[:, r, :] for r in range(share)], axis=0)
    state_b = jnp.concatenate([carry_ref[:, share + r, :] for r in range(share)], axis=0)
    for b in range(chunks):
        before = state_f
        mine_ref[b, :, 0:LANES] = (
            before * jnp.exp(half_ref[2 * b : 2 * b + 1, :])
        ).astype(BF16)
        state_f = state_f * decay_of(b, 0) + upd_ref[2 * b]
    for b in reversed(range(chunks)):
        mine_ref[b, :, LANES : 2 * LANES] = (
            state_b * jnp.exp(half_ref[2 * b + 1 : 2 * b + 2, :])
        ).astype(BF16)
        state_b = state_b * decay_of(b, 1) + upd_ref[2 * b + 1]

    def mix_copy(i):
        peer = lax.rem(row + i, members)
        return pltpu.make_async_remote_copy(
            src_ref=ks_ref.at[peer],
            dst_ref=mixed_ref.at[row],
            send_sem=mix_send_sem.at[i],
            recv_sem=mix_recv_sem.at[i],
            device_id={"tp": peer},
            device_id_type=MESH,
        )

    for b in range(chunks):
        rows = slice(b * CHUNK, (b + 1) * CHUNK)
        across = lax.dot_general(qs_ref[b], mine_ref[b], NT, preferred_element_type=F32)
        for h in range(2):
            o = out_ref[h, rows, :] + across[h * CHUNK : (h + 1) * CHUNK]
            cols = slice(h * DV, (h + 1) * DV)
            o = o * lax.rsqrt(jnp.mean(o * o, axis=-1, keepdims=True) + EPS)
            g = g_ref[rows, cols].astype(F32)
            o = o * gain_ref[0:1, cols] * (g / (1.0 + jnp.exp(-g)))
            ks_ref[b, :, cols] = o.astype(BF16)
    for i in range(1, members):
        mix_copy(i).start()
    send_near(1)
    send_near(2)
    mixed_ref[row] = ks_ref[row]

    expert_id = lax.broadcasted_iota(jnp.int32, (LANES, count), 0)
    earlier_id = lax.broadcasted_iota(jnp.int32, (count, count), 0)
    token_id = lax.broadcasted_iota(jnp.int32, (count, count), 1)
    first_named = routes_ref[0:1, :] == expert_id
    second_named = routes_ref[1:2, :] == expert_id
    named = jnp.where(first_named, 1.0, 0.0) + jnp.where(second_named, 1.0, 0.0)
    earlier = jnp.where(earlier_id < token_id, 1.0, 0.0).astype(BF16)
    rank = jnp.dot(named.astype(BF16), earlier, preferred_element_type=F32)
    ranked = (named * (rank + 1.0)).astype(BF16)
    spread = jnp.dot(spread_ref[...], ranked, preferred_element_type=F32)
    put_ref[...] = jnp.where(spread == target_ref[...], 1.0, 0.0).astype(BF16)

    local_copies[0].wait()
    for i in range(1, members):
        mix_copy(i).wait()
    mixed = jnp.concatenate([mixed_ref[i] for i in range(members)], axis=1)
    step = min(512, width)
    for n in range(width // step):
        cols = slice(n * step, (n + 1) * step)
        total_ref[:, cols] = jnp.dot(mixed, proj_ref[:, cols], preferred_element_type=F32)
    for i in range(count // 16):
        rows = slice(i * 16, (i + 1) * 16)
        p = total_ref[rows, :]
        p = p * lax.rsqrt(jnp.mean(p * p, axis=-1, keepdims=True) + EPS) * mix_gain_ref[...]
        r = (stream_ref[rows, :].astype(F32) + p).astype(BF16)
        residual_ref[rows, :] = r
        r = r.astype(F32)
        r = r * lax.rsqrt(jnp.mean(r * r, axis=-1, keepdims=True) + EPS) * ffn_gain_ref[...]
        normed_ref[rows, :] = r.astype(BF16)

    def piece_of(part, i):
        return pl.ds(pl.multiple_of(part * half_rows + i * piece, 16), piece)

    def row_copy(src, dst, base, part, i):
        peer = peer_of(i)
        return pltpu.make_async_remote_copy(
            src_ref=src.at[piece_of(part, peer)],
            dst_ref=dst.at[piece_of(part, me)],
            send_sem=row_send_sem.at[base + part, offset(i)],
            recv_sem=row_recv_sem.at[base + part, offset(i)],
            device_id={"sp": peer},
            device_id_type=MESH,
        )

    def put_lines(part, line, array):
        for k in range(array.shape[1] // LANES):
            at = pl.ds(part * half_rows + line + k, slots, stride=half_lines)
            stage_ref[at, :] = array[:, k * LANES : (k + 1) * LANES]

    def narrow(part):
        def one(i, c):
            filled_ref[piece_of(part, i), :] = stage_ref[piece_of(part, i), :].astype(BF16)
            return c

        lax.fori_loop(0, groups, one, 0)

    def get_lines(dst, part):
        for k in range(half_lines):
            at = pl.ds(part * half_rows + k, slots, stride=half_lines)
            n = part * half_lines + k
            dst[:, n * LANES : (n + 1) * LANES] = stage_ref[at, :].astype(BF16)

    def send_rows(dst, base, part):
        each(lambda i: row_copy(filled_ref, dst, base, part, i).start())

    def take_rows(dst, base, part):
        own = piece_of(part, me)
        stage_ref[own, :] = filled_ref[own, :].astype(F32)

        def one(i):
            row_copy(filled_ref, dst, base, part, i).wait()
            came = piece_of(part, lax.rem(me + groups - offset(i), groups))
            stage_ref[came, :] = dst[came, :].astype(F32)

        each(one)

    wide = min(2 * LANES, half_width)
    for part in range(2):
        for n in range(half_width // wide):
            cols = pl.ds(part * half_width + n * wide, wide)
            f = jnp.dot(put_ref[...], normed_ref[:, cols], preferred_element_type=F32)
            put_lines(part, n * (wide // LANES), f)
        narrow(part)
        send_rows(arrived_ref, 0, part)

    send_far(1)
    send_near(3)
    send_far(2)
    for t in range(3):
        for side in range(2):
            shared_near(t, side).start()
    for part in range(2):
        take_rows(arrived_ref, 0, part)
    for part in range(2):
        get_lines(x_ref, part)
    for copy in local_copies[1:]:
        copy.wait()

    def hide(slot):
        g = jnp.dot(x_ref[...], gate_all[slot], preferred_element_type=F32)
        u = jnp.dot(x_ref[...], up_all[slot], preferred_element_type=F32)
        hidden_ref[:, slot * inner_width : (slot + 1) * inner_width] = (
            g / (1.0 + jnp.exp(-g)) * u
        ).astype(BF16)

    for slot in range(3):
        hide(slot)
    send_far(3)
    for t in range(2):
        for side in range(2):
            far_copy(t, side).wait_recv()
    hide(3)
    for part in range(2):
        for side in range(2):
            far_copy(2 + part, side).wait_recv()
        for n in range(half_width // wide):
            cols = pl.ds(part * half_width + n * wide, wide)
            f = jnp.dot(hidden_ref[...], down_all[:, cols], preferred_element_type=F32)
            put_lines(part, n * (wide // LANES), f)
        narrow(part)
        send_rows(back_ref, 2, part)

    first_weight = jnp.where(first_named, weight_ref[0:1, :], 0.0)
    weigh = first_weight + jnp.where(second_named, weight_ref[1:2, :], 0.0)
    high = weigh.astype(BF16)
    low = (weigh - high.astype(F32)).astype(BF16)
    put = put_ref[...].astype(F32)
    high = (jnp.dot(spread_ref[...], high, preferred_element_type=F32) * put).astype(BF16)
    low = (jnp.dot(spread_ref[...], low, preferred_element_type=F32) * put).astype(BF16)

    def shared(gate, up, down, first):
        x = normed_ref[...]
        g = jnp.dot(x, gate[...], preferred_element_type=F32)
        u = jnp.dot(x, up[...], preferred_element_type=F32)
        h = (g / (1.0 + jnp.exp(-g)) * u).astype(BF16)
        for n in range(width // step):
            cols = slice(n * step, (n + 1) * step)
            more = jnp.dot(h, down[:, cols], preferred_element_type=F32)
            if first:
                total_ref[:, cols] = more
            else:
                total_ref[:, cols] += more

    for t in range(3):
        for side in range(2):
            shared_near(t, side).wait_recv()
            shared_far(t, side).start()
            twin_copy(t, side, half_of(t, core)).start()
    shared(sgate_ref, sup_ref, sdown_ref, True)
    for t in range(3):
        for side in range(2):
            shared_far(t, side).wait_recv()
        twin_copy(t, 2, half_of(t, core)).start()
    for k in range(3):
        for t in range(3):
            twin_copy(t, k, half_of(t, 1 - core)).wait_recv()
        shared(sgate_all.at[k], sup_all.at[k], sdown_all.at[k], False)
    for t in range(4):
        for side in range(2):
            near_copy(t, side).wait_send()
            far_copy(t, side).wait_send()
    for t in range(3):
        for side in range(2):
            shared_near(t, side).wait_send()
            shared_far(t, side).wait_send()
        for k in range(3):
            twin_copy(t, k, half_of(t, core)).wait_send()

    for part in range(2):
        take_rows(back_ref, 2, part)
        get_lines(x_ref, part)
        for n in range(half_width // wide):
            cols = pl.ds(part * half_width + n * wide, wide)
            total_ref[:, cols] += lax.dot_general(
                high, x_ref[:, cols], TN, preferred_element_type=F32
            ) + lax.dot_general(low, x_ref[:, cols], TN, preferred_element_type=F32)
    for i in range(count // 16):
        rows = slice(i * 16, (i + 1) * 16)
        m = total_ref[rows, :]
        m = m * lax.rsqrt(jnp.mean(m * m, axis=-1, keepdims=True) + EPS) * moe_gain_ref[...]
        updated_ref[rows, :] = (residual_ref[rows, :].astype(F32) + m).astype(BF16)


def slot_tables(experts):
    slot = np.arange(experts * CAP)
    spread = (slot[:, None] // CAP == np.arange(LANES)[None, :]).astype(np.float32)
    target = (slot % CAP + 1).astype(np.float32).reshape(-1, 1)
    return spread, target


def body(
    mesh,
    stream,
    queries,
    key_rows,
    values,
    out_gate,
    fwd_decay,
    bwd_decay,
    head_gain,
    out_proj,
    mix_gain,
    ffn_gain,
    moe_gain,
    routes,
    route_weight,
    expert_gate,
    expert_up,
    expert_down,
    shared_gate,
    shared_up,
    shared_down,
):
    groups, members = mesh.shape["sp"], mesh.shape["tp"]
    span = queries.shape[0]
    chunks = span // CHUNK
    share = DV // groups
    tokens, width = stream.shape
    slots = groups * CAP
    lines = width // LANES
    inner_width = expert_gate.shape[2]
    inner, outer = rope_tables(span, groups)
    spread, target = slot_tables(groups)
    vmem = pl.BlockSpec(memory_space=pltpu.VMEM)
    anywhere = pl.BlockSpec(memory_space=pl.ANY)
    dma = pltpu.SemaphoreType.DMA
    mem = pltpu.VMEM
    return pl.pallas_call(
        functools.partial(layer_kernel, groups, members),
        out_shape=jax.ShapeDtypeStruct((tokens, width), BF16),
        in_specs=[vmem] * 20 + [anywhere] * 4,
        out_specs=vmem,
        scratch_shapes=[
            mem(out_proj.shape, BF16),
            mem((members, width, inner_width), BF16),
            mem((members, width, inner_width), BF16),
            mem((members * inner_width, width), BF16),
            mem((3, *shared_gate.shape), BF16),
            mem((3, *shared_up.shape), BF16),
            mem((3, *shared_down.shape), BF16),
            mem((members, CHUNK, 2 * DV), BF16),
            mem((tokens, width), F32),
            mem((tokens, width), BF16),
            mem((tokens, width), BF16),
            mem((slots, tokens), BF16),
            mem((slots * lines, LANES), F32),
            mem((slots * lines, LANES), BF16),
            mem((slots * lines, LANES), BF16),
            mem((slots * lines, LANES), BF16),
            mem((slots, width), BF16),
            mem((slots, members * inner_width), BF16),
            mem((chunks, 2 * CHUNK, 2 * LANES), BF16),
            mem((chunks, CHUNK, 2 * LANES), BF16),
            mem((2, span, DV), F32),
            mem((2 * chunks, DV, LANES), F32),
            mem((2 * chunks, LANES), F32),
            mem((groups * 4 * share, LANES), F32),
            mem((groups * 4 * share, LANES), F32),
            mem((groups, 2 * share, LANES), F32),
            mem((groups, 2 * share, LANES), F32),
            mem((chunks, DV, 2 * LANES), BF16),
            dma((groups,)),
            dma((groups,)),
            dma((groups,)),
            dma((groups,)),
            dma((members,)),
            dma((members,)),
            dma((4, groups)),
            dma((4, groups)),
            dma((14,)),
            dma((14,)),
            dma((14,)),
            dma((14,)),
            dma((9,)),
            dma((9,)),
            dma((4,)),
        ],
        compiler_params=pltpu.CompilerParams(
            collective_id=0, has_side_effects=True, vmem_limit_bytes=60 * 2**20
        ),
        cost_estimate=pl.CostEstimate(flops=10**10, bytes_accessed=10**8, transcendentals=0),
        name="layer",
    )(
        queries,
        key_rows,
        values,
        out_gate,
        fwd_decay,
        bwd_decay,
        head_gain.reshape(1, -1),
        jnp.asarray(inner),
        jnp.asarray(outer),
        stream,
        mix_gain.reshape(1, -1),
        ffn_gain.reshape(1, -1),
        moe_gain.reshape(1, -1),
        routes.T,
        route_weight.T,
        jnp.asarray(spread).astype(BF16),
        jnp.asarray(target),
        shared_gate,
        shared_up,
        shared_down,
        out_proj,
        expert_gate[0],
        expert_up[0],
        expert_down[0],
    )


def solution(mesh):
    placed = (
        P(("sp", "tp"), None),
        P("sp", "tp"),
        P("sp", "tp"),
        P("sp", "tp"),
        P("sp", "tp"),
        P("sp", "tp"),
        P("sp", "tp"),
        P("tp"),
        P(),
        P(),
        P(),
        P(),
        P(("sp", "tp"), None),
        P(("sp", "tp"), None),
        P("sp", None, "tp"),
        P("sp", None, "tp"),
        P("sp", "tp", None),
        P(None, "tp"),
        P(None, "tp"),
        P("tp", None),
    )
    return jax.shard_map(
        functools.partial(body, mesh),
        mesh=mesh,
        in_specs=placed,
        out_specs=P(("sp", "tp"), None),
        check_vma=False,
    )
```

```python
import functools

import jax
import jax.numpy as jnp
import numpy as np
from jax import lax
from jax.experimental import pallas as pl
from jax.experimental.pallas import tpu as pltpu
from jax.sharding import PartitionSpec as P

KEY_CHANNELS = 64
DV = 128
TOPK = 2
CAP = 6
CHUNK = 128
LANES = 128
EPS = 1e-06
GATE_NORM = 16.0
ROPE_BASE = 10000.0
MESH = pl.DeviceIdType.MESH
NT = (((1,), (1,)), ((), ()))
TN = (((0,), (0,)), ((), ()))
F32 = jnp.float32
BF16 = jnp.bfloat16


def rope_tables(span, devices):
    half = KEY_CHANNELS // 2
    freq = ROPE_BASE ** (-np.arange(half, dtype=np.float64) / half)
    freq = np.tile(freq, LANES // half)
    inner = np.arange(span)[:, None] * freq[None, :]
    outer = (np.arange(devices) * span)[:, None] * freq[None, :]
    inner = np.stack([np.cos(inner), np.sin(inner)]).astype(np.float32)
    outer = np.stack([np.cos(outer), np.sin(outer)], axis=1).astype(np.float32)
    return inner, outer


def layer_kernel(
    groups,
    members,
    q_ref,
    k_ref,
    v_ref,
    g_ref,
    fd_ref,
    bd_ref,
    gain_ref,
    inner_ref,
    outer_ref,
    stream_ref,
    mix_gain_ref,
    ffn_gain_ref,
    moe_gain_ref,
    routes_ref,
    weight_ref,
    spread_ref,
    target_ref,
    sgate_ref,
    sup_ref,
    sdown_ref,
    proj_hbm,
    gate_hbm,
    up_hbm,
    down_hbm,
    updated_ref,
    proj_ref,
    gate_all,
    up_all,
    down_all,
    sgate_all,
    sup_all,
    sdown_all,
    mixed_ref,
    total_ref,
    residual_ref,
    normed_ref,
    put_ref,
    stage_ref,
    filled_ref,
    arrived_ref,
    back_ref,
    x_ref,
    hidden_ref,
    qs_ref,
    ks_ref,
    out_ref,
    upd_ref,
    half_ref,
    send_ref,
    got_ref,
    back_state_ref,
    carry_ref,
    mine_ref,
    send_sem,
    recv_sem,
    back_send_sem,
    back_recv_sem,
    mix_send_sem,
    mix_recv_sem,
    row_send_sem,
    row_recv_sem,
    near_send_sem,
    near_recv_sem,
    far_send_sem,
    far_recv_sem,
    cross_send_sem,
    cross_recv_sem,
    twin_send_sem,
    twin_recv_sem,
    local_sem,
):
    me = lax.axis_index("sp")
    row = lax.axis_index("tp")
    core = lax.rem(me, 2)
    twin = me + 1 - 2 * core
    span = q_ref.shape[0]
    chunks = span // CHUNK
    share = DV // groups
    message = 4 * share
    count, width = stream_ref.shape
    lines = width // LANES
    slots = put_ref.shape[0]
    half_lines = lines // 2
    half_rows = slots * half_lines
    piece = half_rows // groups
    inner_width = gate_hbm.shape[1]
    sides = (lax.rem(row + 1, members), lax.rem(row + members - 1, members))

    barrier = pltpu.get_barrier_semaphore()

    def greet(i, c):
        pl.semaphore_signal(
            barrier, inc=1, device_id={"sp": lax.rem(me + i, groups)}, device_id_type=MESH
        )
        return c

    lax.fori_loop(1, groups, greet, 0)
    for i in range(1, members):
        pl.semaphore_signal(
            barrier, inc=1, device_id={"tp": lax.rem(row + i, members)}, device_id_type=MESH
        )

    own_down = pl.ds(0, inner_width)
    local_copies = [
        pltpu.make_async_copy(proj_hbm, proj_ref, local_sem.at[0]),
        pltpu.make_async_copy(gate_hbm, gate_all.at[0], local_sem.at[1]),
        pltpu.make_async_copy(up_hbm, up_all.at[0], local_sem.at[2]),
        pltpu.make_async_copy(down_hbm, down_all.at[own_down], local_sem.at[3]),
    ]
    for copy in local_copies:
        copy.start()

    half_width = width // 2

    def place(t, slot, start, size):
        if t < 2:
            whole = (gate_all, up_all)[t]
            return whole.at[slot, pl.ds(start, size)]
        cols = pl.ds((t - 2) * half_width, half_width)
        return down_all.at[pl.ds(slot * inner_width + start, size), cols]

    def shard(t):
        if t < 2:
            return (gate_hbm, up_hbm)[t]
        return down_hbm.at[:, pl.ds((t - 2) * half_width, half_width)]

    def depth(t):
        return width if t < 2 else inner_width

    def near_copy(t, side):
        return pltpu.make_async_remote_copy(
            src_ref=shard(t),
            dst_ref=place(t, 1 + side, 0, depth(t)),
            send_sem=near_send_sem.at[2 * t + side],
            recv_sem=near_recv_sem.at[2 * t + side],
            device_id={"tp": sides[side]},
            device_id_type=MESH,
        )

    def far_copy(t, side, sub):
        h = depth(t) // 4
        start = (2 * side + sub) * h
        return pltpu.make_async_remote_copy(
            src_ref=place(t, 1 + side, start, h),
            dst_ref=place(t, 3, start, h),
            send_sem=far_send_sem.at[4 * t + 2 * side + sub],
            recv_sem=far_recv_sem.at[4 * t + 2 * side + sub],
            device_id={"tp": sides[side]},
            device_id_type=MESH,
        )

    def send_near(t):
        for side in range(2):
            near_copy(t, side).start()

    def take_near(t):
        for side in range(2):
            near_copy(t, side).wait_recv()

    def send_far(t, subs=(0, 1)):
        for side in range(2):
            for sub in subs:
                far_copy(t, side, sub).start()

    shared_own = (sgate_ref, sup_ref, sdown_ref)
    shared_all = (sgate_all, sup_all, sdown_all)

    crew = min(8, groups)
    seat = lax.rem(me, crew)
    stops = crew // 2
    turn = core * stops + lax.div(seat, 2)

    def half_of(t, who):
        h = shared_own[t].shape[0] // 2
        return pl.ds(pl.multiple_of(who * h, 16), h)

    def share_of(t):
        e = shared_own[t].shape[0] // crew
        return pl.ds(pl.multiple_of(turn * e, 16), e)

    def shared_near(t, side):
        return pltpu.make_async_remote_copy(
            src_ref=shared_own[t].at[share_of(t)],
            dst_ref=shared_all[t].at[side, share_of(t)],
            send_sem=near_send_sem.at[8 + 2 * t + side],
            recv_sem=near_recv_sem.at[8 + 2 * t + side],
            device_id={"tp": sides[side]},
            device_id_type=MESH,
        )

    def part_of(t, k, side):
        if t < 2:
            e = shared_own[t].shape[0] // crew
            start = pl.multiple_of(turn * e + side * (e // 2), 16)
            return shared_all[t].at[k, pl.ds(start, e // 2)]
        return shared_all[t].at[k, share_of(t), pl.ds(side * half_width, half_width)]

    def shared_far(t, side):
        return pltpu.make_async_remote_copy(
            src_ref=part_of(t, side, side),
            dst_ref=part_of(t, 2, side),
            send_sem=far_send_sem.at[16 + 2 * t + side],
            recv_sem=far_recv_sem.at[16 + 2 * t + side],
            device_id={"tp": sides[side]},
            device_id_type=MESH,
        )

    def cross_copy(t, k, n):
        return pltpu.make_async_remote_copy(
            src_ref=shared_all[t].at[k, share_of(t)],
            dst_ref=shared_all[t].at[k, share_of(t)],
            send_sem=cross_send_sem.at[(3 * t + k) * stops + n],
            recv_sem=cross_recv_sem.at[(3 * t + k) * stops + n],
            device_id={"sp": me - seat + lax.rem(seat + 2 * n, crew)},
            device_id_type=MESH,
        )

    def send_cross(k):
        for t in range(3):
            for n in range(1, stops):
                cross_copy(t, k, n).start()

    def twin_copy(t, k, part):
        return pltpu.make_async_remote_copy(
            src_ref=shared_all[t].at[k, part],
            dst_ref=shared_all[t].at[k, part],
            send_sem=twin_send_sem.at[3 * t + k],
            recv_sem=twin_recv_sem.at[3 * t + k],
            device_id={"sp": twin},
            device_id_type=MESH,
        )

    lane = lax.broadcasted_iota(jnp.int32, (CHUNK, LANES), 1)
    r_id = lax.broadcasted_iota(jnp.int32, (CHUNK, CHUNK), 0)
    c_id = lax.broadcasted_iota(jnp.int32, (CHUNK, CHUNK), 1)
    lower = r_id >= c_id
    upper = r_id <= c_id
    lower_one = jnp.where(lower, 1.0, 0.0).astype(BF16)
    upper_one = jnp.where(upper, 1.0, 0.0).astype(BF16)
    front = (lane % KEY_CHANNELS) < (KEY_CHANNELS // 2)
    first_head = lane < KEY_CHANNELS
    cos_0 = outer_ref[me, 0:1, :]
    sin_0 = outer_ref[me, 1:2, :]

    def log_decay(x):
        return (jnp.minimum(x, 0.0) - jnp.log1p(jnp.exp(-jnp.abs(x)))) * (1.0 / GATE_NORM)

    def cumulate(tri, x):
        high = x.astype(BF16)
        low = (x - high.astype(F32)).astype(BF16)
        return jnp.dot(tri, high, preferred_element_type=F32) + jnp.dot(
            tri, low, preferred_element_type=F32
        )

    for b in range(chunks):
        rows = slice(b * CHUNK, (b + 1) * CHUNK)
        cos_i = inner_ref[0, rows, :]
        sin_i = inner_ref[1, rows, :]
        cosine = cos_0 * cos_i - sin_0 * sin_i
        sine = sin_0 * cos_i + cos_0 * sin_i
        sine = jnp.where(front, -sine, sine)

        def rotated(u):
            swapped = jnp.where(
                front,
                pltpu.roll(u, LANES - KEY_CHANNELS // 2, 1),
                pltpu.roll(u, KEY_CHANNELS // 2, 1),
            )
            return u * cosine + swapped * sine

        q = rotated(q_ref[rows, :].astype(F32) * KEY_CHANNELS ** (-0.5))
        k = rotated(k_ref[rows, :].astype(F32))
        cf = cumulate(lower_one, log_decay(fd_ref[rows, :]))
        cb = cumulate(upper_one, log_decay(bd_ref[rows, :]))
        hf = cf[CHUNK - 1 : CHUNK, :] * 0.5
        hb = cb[0:1, :] * 0.5
        half_ref[2 * b : 2 * b + 1, :] = hf
        half_ref[2 * b + 1 : 2 * b + 2, :] = hb
        qf = q * jnp.exp(cf - hf)
        qb = q * jnp.exp(cb - hb)
        kf = (k * jnp.exp(hf - cf)).astype(BF16)
        kb = (k * jnp.exp(hb - cb)).astype(BF16)
        ks_ref[b, :, 0:LANES] = kf
        ks_ref[b, :, LANES : 2 * LANES] = kb
        qs_ref[b, 0:CHUNK, 0:LANES] = jnp.where(first_head, qf, 0.0).astype(BF16)
        qs_ref[b, 0:CHUNK, LANES : 2 * LANES] = jnp.where(first_head, qb, 0.0).astype(BF16)
        qs_ref[b, CHUNK : 2 * CHUNK, 0:LANES] = jnp.where(first_head, 0.0, qf).astype(BF16)
        qs_ref[b, CHUNK : 2 * CHUNK, LANES : 2 * LANES] = jnp.where(first_head, 0.0, qb).astype(
            BF16
        )
        both = lax.dot_general(
            v_ref[rows, :], ks_ref[b], TN, preferred_element_type=F32
        )
        upd_ref[2 * b] = jnp.where(
            first_head, both[0:DV, 0:LANES], both[DV : 2 * DV, 0:LANES]
        ) * jnp.exp(hf)
        upd_ref[2 * b + 1] = jnp.where(
            first_head, both[0:DV, LANES : 2 * LANES], both[DV : 2 * DV, LANES : 2 * LANES]
        ) * jnp.exp(hb)
        if b == 0:
            pl.semaphore_wait(barrier, groups - 1 + members - 1)
            for t in range(3):
                for side in range(2):
                    shared_near(t, side).start()
            send_near(0)

    def decay_of(b, d):
        return jnp.exp(half_ref[2 * b + d : 2 * b + d + 1, :] * 2.0)

    total_f = upd_ref[0]
    decay_f = decay_of(0, 0)
    for b in range(1, chunks):
        total_f = total_f * decay_of(b, 0) + upd_ref[2 * b]
        decay_f = decay_f * decay_of(b, 0)
    total_b = upd_ref[2 * (chunks - 1) + 1]
    decay_b = decay_of(chunks - 1, 1)
    for b in reversed(range(chunks - 1)):
        total_b = total_b * decay_of(b, 1) + upd_ref[2 * b + 1]
        decay_b = decay_b * decay_of(b, 1)
    for r in range(share):
        part = slice(r * groups, (r + 1) * groups)
        send_ref[pl.ds(r, groups, stride=message), :] = total_f[part, :]
        send_ref[pl.ds(share + r, groups, stride=message), :] = total_b[part, :]
        send_ref[pl.ds(2 * share + r, groups, stride=message), :] = jnp.broadcast_to(
            decay_f, (groups, LANES)
        )
        send_ref[pl.ds(3 * share + r, groups, stride=message), :] = jnp.broadcast_to(
            decay_b, (groups, LANES)
        )

    def block(ref, i):
        return ref.at[pl.ds(pl.multiple_of(i * message, message), message)]

    def half_block(ref, i):
        return ref.at[i]

    def out_copy(peer, i):
        return pltpu.make_async_remote_copy(
            src_ref=block(send_ref, peer),
            dst_ref=block(got_ref, me),
            send_sem=send_sem.at[i],
            recv_sem=recv_sem.at[i],
            device_id={"sp": peer},
            device_id_type=MESH,
        )

    def back_copy(peer, i):
        return pltpu.make_async_remote_copy(
            src_ref=half_block(back_state_ref, peer),
            dst_ref=half_block(carry_ref, me),
            send_sem=back_send_sem.at[i],
            recv_sem=back_recv_sem.at[i],
            device_id={"sp": peer},
            device_id_type=MESH,
        )

    def offset(i):
        half = lax.div(i + 1, 2)
        return jnp.where(lax.rem(i, 2) == 1, half, groups - half)

    def peer_of(i):
        return lax.rem(me + offset(i), groups)

    def each(action):
        def step(i, c):
            action(i)
            return c

        lax.fori_loop(1, groups, step, 0)

    each(lambda i: out_copy(peer_of(i), offset(i)).start())
    for t in range(3):
        for side in range(2):
            shared_near(t, side).wait_recv()
            shared_far(t, side).start()
    send_cross(0)
    mine = pl.ds(pl.multiple_of(me * message, message), message)
    got_ref[mine, :] = send_ref[mine, :]

    for b in range(chunks):
        rows = slice(b * CHUNK, (b + 1) * CHUNK)
        s_f = lax.dot_general(
            qs_ref[b, :, 0:LANES], ks_ref[b, :, 0:LANES], NT, preferred_element_type=F32
        )
        s_b = lax.dot_general(
            qs_ref[b, :, LANES : 2 * LANES],
            ks_ref[b, :, LANES : 2 * LANES],
            NT,
            preferred_element_type=F32,
        )
        for h in range(2):
            part = slice(h * CHUNK, (h + 1) * CHUNK)
            s = jnp.where(lower, s_f[part], 0.0) + jnp.where(upper, s_b[part], 0.0)
            out_ref[h, rows, :] = jnp.dot(
                s.astype(BF16), v_ref[rows, h * DV : (h + 1) * DV], preferred_element_type=F32
            )

    each(lambda i: out_copy(peer_of(i), offset(i)).wait())

    zero = jnp.zeros((share, LANES), F32)

    def scan(s, carried):
        c_f, c_b = carried
        t = groups - 1 - s
        at_s = pl.multiple_of(s * message, message)
        at_t = pl.multiple_of(t * message, message)
        m_s = got_ref[pl.ds(at_s, message), :]
        m_t = got_ref[pl.ds(at_t, message), :]
        back_state_ref[s, 0:share, :] = c_f
        back_state_ref[t, share : 2 * share, :] = c_b
        c_f = c_f * m_s[2 * share : 3 * share] + m_s[0:share]
        c_b = c_b * m_t[3 * share : 4 * share] + m_t[share : 2 * share]
        return c_f, c_b

    lax.fori_loop(0, groups, scan, (zero, zero))
    each(lambda i: back_copy(peer_of(i), offset(i)).start())
    carry_ref[me] = back_state_ref[me]
    send_cross(1)
    take_near(0)
    send_far(0, (0,))
    each(lambda i: back_copy(peer_of(i), offset(i)).wait())

    state_f = jnp.concatenate([carry_ref[:, r, :] for r in range(share)], axis=0)
    state_b = jnp.concatenate([carry_ref[:, share + r, :] for r in range(share)], axis=0)
    for b in range(chunks):
        before = state_f
        mine_ref[b, :, 0:LANES] = (
            before * jnp.exp(half_ref[2 * b : 2 * b + 1, :])
        ).astype(BF16)
        state_f = state_f * decay_of(b, 0) + upd_ref[2 * b]
    for b in reversed(range(chunks)):
        mine_ref[b, :, LANES : 2 * LANES] = (
            state_b * jnp.exp(half_ref[2 * b + 1 : 2 * b + 2, :])
        ).astype(BF16)
        state_b = state_b * decay_of(b, 1) + upd_ref[2 * b + 1]

    def mix_copy(i):
        peer = lax.rem(row + i, members)
        return pltpu.make_async_remote_copy(
            src_ref=ks_ref.at[peer],
            dst_ref=mixed_ref.at[row],
            send_sem=mix_send_sem.at[i],
            recv_sem=mix_recv_sem.at[i],
            device_id={"tp": peer},
            device_id_type=MESH,
        )

    for b in range(chunks):
        rows = slice(b * CHUNK, (b + 1) * CHUNK)
        across = lax.dot_general(qs_ref[b], mine_ref[b], NT, preferred_element_type=F32)
        for h in range(2):
            o = out_ref[h, rows, :] + across[h * CHUNK : (h + 1) * CHUNK]
            cols = slice(h * DV, (h + 1) * DV)
            o = o * lax.rsqrt(jnp.mean(o * o, axis=-1, keepdims=True) + EPS)
            g = g_ref[rows, cols].astype(F32)
            o = o * gain_ref[0:1, cols] * (g / (1.0 + jnp.exp(-g)))
            ks_ref[b, :, cols] = o.astype(BF16)
    for i in range(1, members):
        mix_copy(i).start()
    send_near(1)
    send_near(2)
    send_far(0, (1,))
    for t in range(3):
        for side in range(2):
            shared_far(t, side).wait_recv()
    send_cross(2)
    mixed_ref[row] = ks_ref[row]

    expert_id = lax.broadcasted_iota(jnp.int32, (LANES, count), 0)
    earlier_id = lax.broadcasted_iota(jnp.int32, (count, count), 0)
    token_id = lax.broadcasted_iota(jnp.int32, (count, count), 1)
    first_named = routes_ref[0:1, :] == expert_id
    second_named = routes_ref[1:2, :] == expert_id
    named = jnp.where(first_named, 1.0, 0.0) + jnp.where(second_named, 1.0, 0.0)
    earlier = jnp.where(earlier_id < token_id, 1.0, 0.0).astype(BF16)
    rank = jnp.dot(named.astype(BF16), earlier, preferred_element_type=F32)
    ranked = (named * (rank + 1.0)).astype(BF16)
    spread = jnp.dot(spread_ref[...], ranked, preferred_element_type=F32)
    put_ref[...] = jnp.where(spread == target_ref[...], 1.0, 0.0).astype(BF16)

    local_copies[0].wait()
    for i in range(1, members):
        mix_copy(i).wait()
    mixed = jnp.concatenate([mixed_ref[i] for i in range(members)], axis=1)
    step = min(512, width)
    for n in range(width // step):
        cols = slice(n * step, (n + 1) * step)
        total_ref[:, cols] = jnp.dot(mixed, proj_ref[:, cols], preferred_element_type=F32)
    for i in range(count // 16):
        rows = slice(i * 16, (i + 1) * 16)
        p = total_ref[rows, :]
        p = p * lax.rsqrt(jnp.mean(p * p, axis=-1, keepdims=True) + EPS) * mix_gain_ref[...]
        r = (stream_ref[rows, :].astype(F32) + p).astype(BF16)
        residual_ref[rows, :] = r
        r = r.astype(F32)
        r = r * lax.rsqrt(jnp.mean(r * r, axis=-1, keepdims=True) + EPS) * ffn_gain_ref[...]
        normed_ref[rows, :] = r.astype(BF16)

    def piece_of(part, i):
        return pl.ds(pl.multiple_of(part * half_rows + i * piece, 16), piece)

    def row_copy(src, dst, base, part, i):
        peer = peer_of(i)
        return pltpu.make_async_remote_copy(
            src_ref=src.at[piece_of(part, peer)],
            dst_ref=dst.at[piece_of(part, me)],
            send_sem=row_send_sem.at[base + part, offset(i)],
            recv_sem=row_recv_sem.at[base + part, offset(i)],
            device_id={"sp": peer},
            device_id_type=MESH,
        )

    def put_lines(part, line, array):
        for k in range(array.shape[1] // LANES):
            at = pl.ds(part * half_rows + line + k, slots, stride=half_lines)
            stage_ref[at, :] = array[:, k * LANES : (k + 1) * LANES]

    def narrow(part):
        def one(i, c):
            filled_ref[piece_of(part, i), :] = stage_ref[piece_of(part, i), :].astype(BF16)
            return c

        lax.fori_loop(0, groups, one, 0)

    def get_lines(dst, part):
        for k in range(half_lines):
            at = pl.ds(part * half_rows + k, slots, stride=half_lines)
            n = part * half_lines + k
            dst[:, n * LANES : (n + 1) * LANES] = stage_ref[at, :].astype(BF16)

    def send_rows(dst, base, part):
        each(lambda i: row_copy(filled_ref, dst, base, part, i).start())

    def take_rows(dst, base, part):
        own = piece_of(part, me)
        stage_ref[own, :] = filled_ref[own, :].astype(F32)

        def one(i):
            row_copy(filled_ref, dst, base, part, i).wait()
            came = piece_of(part, lax.rem(me + groups - offset(i), groups))
            stage_ref[came, :] = dst[came, :].astype(F32)

        each(one)

    wide = min(2 * LANES, half_width)
    for part in range(2):
        for n in range(half_width // wide):
            cols = pl.ds(part * half_width + n * wide, wide)
            f = jnp.dot(put_ref[...], normed_ref[:, cols], preferred_element_type=F32)
            put_lines(part, n * (wide // LANES), f)
        narrow(part)
        send_rows(arrived_ref, 0, part)

    def shared(gate, up, down, first):
        x = normed_ref[...]
        g = jnp.dot(x, gate[...], preferred_element_type=F32)
        u = jnp.dot(x, up[...], preferred_element_type=F32)
        h = (g / (1.0 + jnp.exp(-g)) * u).astype(BF16)
        for n in range(width // step):
            cols = slice(n * step, (n + 1) * step)
            more = jnp.dot(h, down[:, cols], preferred_element_type=F32)
            if first:
                total_ref[:, cols] = more
            else:
                total_ref[:, cols] += more

    for t in range(3):
        for k in range(3):
            for n in range(1, stops):
                cross_copy(t, k, n).wait_recv()
            twin_copy(t, k, half_of(t, core)).start()
    take_near(1)
    send_far(1)
    take_near(2)
    send_far(2)
    send_near(3)
    shared(sgate_ref, sup_ref, sdown_ref, True)
    for k in range(3):
        for t in range(3):
            twin_copy(t, k, half_of(t, 1 - core)).wait_recv()
        shared(sgate_all.at[k], sup_all.at[k], sdown_all.at[k], False)
    for part in range(2):
        take_rows(arrived_ref, 0, part)
    for part in range(2):
        get_lines(x_ref, part)
    for copy in local_copies[1:]:
        copy.wait()

    def hide(slot):
        g = jnp.dot(x_ref[...], gate_all[slot], preferred_element_type=F32)
        u = jnp.dot(x_ref[...], up_all[slot], preferred_element_type=F32)
        hidden_ref[:, slot * inner_width : (slot + 1) * inner_width] = (
            g / (1.0 + jnp.exp(-g)) * u
        ).astype(BF16)

    for slot in range(3):
        hide(slot)
    for t in range(2):
        for side in range(2):
            for sub in range(2):
                far_copy(t, side, sub).wait_recv()
    hide(3)
    for part in range(2):
        if part == 1:
            take_near(3)
            send_far(3)
        for side in range(2):
            for sub in range(2):
                far_copy(2 + part, side, sub).wait_recv()
        for n in range(half_width // wide):
            cols = pl.ds(part * half_width + n * wide, wide)
            f = jnp.dot(hidden_ref[...], down_all[:, cols], preferred_element_type=F32)
            put_lines(part, n * (wide // LANES), f)
        narrow(part)
        send_rows(back_ref, 2, part)

    first_weight = jnp.where(first_named, weight_ref[0:1, :], 0.0)
    weigh = first_weight + jnp.where(second_named, weight_ref[1:2, :], 0.0)
    high = weigh.astype(BF16)
    low = (weigh - high.astype(F32)).astype(BF16)
    put = put_ref[...].astype(F32)
    high = (jnp.dot(spread_ref[...], high, preferred_element_type=F32) * put).astype(BF16)
    low = (jnp.dot(spread_ref[...], low, preferred_element_type=F32) * put).astype(BF16)

    for t in range(4):
        for side in range(2):
            near_copy(t, side).wait_send()
            for sub in range(2):
                far_copy(t, side, sub).wait_send()
    for t in range(3):
        for side in range(2):
            shared_near(t, side).wait_send()
            shared_far(t, side).wait_send()
        for k in range(3):
            for n in range(1, stops):
                cross_copy(t, k, n).wait_send()
            twin_copy(t, k, half_of(t, core)).wait_send()

    for part in range(2):
        take_rows(back_ref, 2, part)
        get_lines(x_ref, part)
        for n in range(half_width // wide):
            cols = pl.ds(part * half_width + n * wide, wide)
            total_ref[:, cols] += lax.dot_general(
                high, x_ref[:, cols], TN, preferred_element_type=F32
            ) + lax.dot_general(low, x_ref[:, cols], TN, preferred_element_type=F32)
    for i in range(count // 16):
        rows = slice(i * 16, (i + 1) * 16)
        m = total_ref[rows, :]
        m = m * lax.rsqrt(jnp.mean(m * m, axis=-1, keepdims=True) + EPS) * moe_gain_ref[...]
        updated_ref[rows, :] = (residual_ref[rows, :].astype(F32) + m).astype(BF16)


def slot_tables(experts):
    slot = np.arange(experts * CAP)
    spread = (slot[:, None] // CAP == np.arange(LANES)[None, :]).astype(np.float32)
    target = (slot % CAP + 1).astype(np.float32).reshape(-1, 1)
    return spread, target


def body(
    mesh,
    stream,
    queries,
    key_rows,
    values,
    out_gate,
    fwd_decay,
    bwd_decay,
    head_gain,
    out_proj,
    mix_gain,
    ffn_gain,
    moe_gain,
    routes,
    route_weight,
    expert_gate,
    expert_up,
    expert_down,
    shared_gate,
    shared_up,
    shared_down,
):
    groups, members = mesh.shape["sp"], mesh.shape["tp"]
    span = queries.shape[0]
    chunks = span // CHUNK
    share = DV // groups
    tokens, width = stream.shape
    slots = groups * CAP
    lines = width // LANES
    inner_width = expert_gate.shape[2]
    inner, outer = rope_tables(span, groups)
    spread, target = slot_tables(groups)
    vmem = pl.BlockSpec(memory_space=pltpu.VMEM)
    anywhere = pl.BlockSpec(memory_space=pl.ANY)
    dma = pltpu.SemaphoreType.DMA
    mem = pltpu.VMEM
    return pl.pallas_call(
        functools.partial(layer_kernel, groups, members),
        out_shape=jax.ShapeDtypeStruct((tokens, width), BF16),
        in_specs=[vmem] * 20 + [anywhere] * 4,
        out_specs=vmem,
        scratch_shapes=[
            mem(out_proj.shape, BF16),
            mem((members, width, inner_width), BF16),
            mem((members, width, inner_width), BF16),
            mem((members * inner_width, width), BF16),
            mem((3, *shared_gate.shape), BF16),
            mem((3, *shared_up.shape), BF16),
            mem((3, *shared_down.shape), BF16),
            mem((members, CHUNK, 2 * DV), BF16),
            mem((tokens, width), F32),
            mem((tokens, width), BF16),
            mem((tokens, width), BF16),
            mem((slots, tokens), BF16),
            mem((slots * lines, LANES), F32),
            mem((slots * lines, LANES), BF16),
            mem((slots * lines, LANES), BF16),
            mem((slots * lines, LANES), BF16),
            mem((slots, width), BF16),
            mem((slots, members * inner_width), BF16),
            mem((chunks, 2 * CHUNK, 2 * LANES), BF16),
            mem((chunks, CHUNK, 2 * LANES), BF16),
            mem((2, span, DV), F32),
            mem((2 * chunks, DV, LANES), F32),
            mem((2 * chunks, LANES), F32),
            mem((groups * 4 * share, LANES), F32),
            mem((groups * 4 * share, LANES), F32),
            mem((groups, 2 * share, LANES), F32),
            mem((groups, 2 * share, LANES), F32),
            mem((chunks, DV, 2 * LANES), BF16),
            dma((groups,)),
            dma((groups,)),
            dma((groups,)),
            dma((groups,)),
            dma((members,)),
            dma((members,)),
            dma((4, groups)),
            dma((4, groups)),
            dma((14,)),
            dma((14,)),
            dma((22,)),
            dma((22,)),
            dma((9 * min(4, groups // 2),)),
            dma((9 * min(4, groups // 2),)),
            dma((9,)),
            dma((9,)),
            dma((4,)),
        ],
        compiler_params=pltpu.CompilerParams(
            collective_id=0, has_side_effects=True, vmem_limit_bytes=60 * 2**20
        ),
        cost_estimate=pl.CostEstimate(flops=10**10, bytes_accessed=10**8, transcendentals=0),
        name="layer",
    )(
        queries,
        key_rows,
        values,
        out_gate,
        fwd_decay,
        bwd_decay,
        head_gain.reshape(1, -1),
        jnp.asarray(inner),
        jnp.asarray(outer),
        stream,
        mix_gain.reshape(1, -1),
        ffn_gain.reshape(1, -1),
        moe_gain.reshape(1, -1),
        routes.T,
        route_weight.T,
        jnp.asarray(spread).astype(BF16),
        jnp.asarray(target),
        shared_gate,
        shared_up,
        shared_down,
        out_proj,
        expert_gate[0],
        expert_up[0],
        expert_down[0],
    )


def solution(mesh):
    placed = (
        P(("sp", "tp"), None),
        P("sp", "tp"),
        P("sp", "tp"),
        P("sp", "tp"),
        P("sp", "tp"),
        P("sp", "tp"),
        P("sp", "tp"),
        P("tp"),
        P(),
        P(),
        P(),
        P(),
        P(("sp", "tp"), None),
        P(("sp", "tp"), None),
        P("sp", None, "tp"),
        P("sp", None, "tp"),
        P("sp", "tp", None),
        P(None, "tp"),
        P(None, "tp"),
        P("tp", None),
    )
    return jax.shard_map(
        functools.partial(body, mesh),
        mesh=mesh,
        in_specs=placed,
        out_specs=P(("sp", "tp"), None),
        check_vma=False,
    )
```

```python
import functools

import jax
import jax.numpy as jnp
import numpy as np
from jax import lax
from jax.experimental import pallas as pl
from jax.experimental.pallas import tpu as pltpu
from jax.sharding import PartitionSpec as P

KEY_CHANNELS = 64
DV = 128
TOPK = 2
CAP = 6
CHUNK = 128
OUT_PARTS = ((0, 16),)
BACK_PARTS = ((0, 8), (8, 8))
EARLY = 3
LANES = 128
EPS = 1e-06
GATE_NORM = 16.0
ROPE_BASE = 10000.0
MESH = pl.DeviceIdType.MESH
NT = (((1,), (1,)), ((), ()))
TN = (((0,), (0,)), ((), ()))
F32 = jnp.float32
BF16 = jnp.bfloat16


def rope_tables(span, devices):
    half = KEY_CHANNELS // 2
    freq = ROPE_BASE ** (-np.arange(half, dtype=np.float64) / half)
    freq = np.tile(freq, LANES // half)
    inner = np.arange(span)[:, None] * freq[None, :]
    outer = (np.arange(devices) * span)[:, None] * freq[None, :]
    inner = np.stack([np.cos(inner), np.sin(inner)]).astype(np.float32)
    outer = np.stack([np.cos(outer), np.sin(outer)], axis=1).astype(np.float32)
    return inner, outer


def layer_kernel(
    groups,
    members,
    q_ref,
    k_ref,
    v_ref,
    g_ref,
    fd_ref,
    bd_ref,
    gain_ref,
    inner_ref,
    outer_ref,
    stream_ref,
    mix_gain_ref,
    ffn_gain_ref,
    moe_gain_ref,
    routes_ref,
    weight_ref,
    spread_ref,
    target_ref,
    sgate_ref,
    sup_ref,
    sdown_ref,
    proj_hbm,
    gate_hbm,
    up_hbm,
    down_hbm,
    updated_ref,
    proj_ref,
    gate_all,
    up_all,
    down_all,
    sgate_all,
    sup_all,
    sdown_all,
    mixed_ref,
    total_ref,
    residual_ref,
    normed_ref,
    put_ref,
    stage_ref,
    filled_ref,
    arrived_ref,
    back_ref,
    x_ref,
    hidden_ref,
    qs_ref,
    ks_ref,
    out_ref,
    upd_ref,
    half_ref,
    send_ref,
    got_ref,
    back_state_ref,
    carry_ref,
    mine_ref,
    send_sem,
    recv_sem,
    back_send_sem,
    back_recv_sem,
    mix_send_sem,
    mix_recv_sem,
    row_send_sem,
    row_recv_sem,
    near_send_sem,
    near_recv_sem,
    far_send_sem,
    far_recv_sem,
    cross_send_sem,
    cross_recv_sem,
    twin_send_sem,
    twin_recv_sem,
    local_sem,
):
    me = lax.axis_index("sp")
    row = lax.axis_index("tp")
    core = lax.rem(me, 2)
    twin = me + 1 - 2 * core
    span = q_ref.shape[0]
    chunks = span // CHUNK
    share = DV // groups
    message = 4 * share
    count, width = stream_ref.shape
    lines = width // LANES
    slots = put_ref.shape[0]
    inner_width = gate_hbm.shape[1]
    sides = (lax.rem(row + 1, members), lax.rem(row + members - 1, members))

    barrier = pltpu.get_barrier_semaphore()

    def greet(i, c):
        pl.semaphore_signal(
            barrier, inc=1, device_id={"sp": lax.rem(me + i, groups)}, device_id_type=MESH
        )
        return c

    lax.fori_loop(1, groups, greet, 0)
    for i in range(1, members):
        pl.semaphore_signal(
            barrier, inc=1, device_id={"tp": lax.rem(row + i, members)}, device_id_type=MESH
        )

    own_down = pl.ds(0, inner_width)
    local_copies = [
        pltpu.make_async_copy(proj_hbm, proj_ref, local_sem.at[0]),
        pltpu.make_async_copy(gate_hbm, gate_all.at[0], local_sem.at[1]),
        pltpu.make_async_copy(up_hbm, up_all.at[0], local_sem.at[2]),
        pltpu.make_async_copy(down_hbm, down_all.at[own_down], local_sem.at[3]),
    ]
    for copy in local_copies:
        copy.start()

    half_width = width // 2

    def columns_of(t):
        first, number = BACK_PARTS[t - 2]
        return pl.ds(first * LANES, number * LANES)

    def place(t, slot, start, size):
        if t < 2:
            whole = (gate_all, up_all)[t]
            return whole.at[slot, pl.ds(start, size)]
        cols = columns_of(t)
        return down_all.at[pl.ds(slot * inner_width + start, size), cols]

    def shard(t):
        if t < 2:
            return (gate_hbm, up_hbm)[t]
        return down_hbm.at[:, columns_of(t)]

    def depth(t):
        return width if t < 2 else inner_width

    def near_copy(t, side):
        return pltpu.make_async_remote_copy(
            src_ref=shard(t),
            dst_ref=place(t, 1 + side, 0, depth(t)),
            send_sem=near_send_sem.at[2 * t + side],
            recv_sem=near_recv_sem.at[2 * t + side],
            device_id={"tp": sides[side]},
            device_id_type=MESH,
        )

    def far_copy(t, side, sub):
        h = depth(t) // 4
        start = (2 * side + sub) * h
        return pltpu.make_async_remote_copy(
            src_ref=place(t, 1 + side, start, h),
            dst_ref=place(t, 3, start, h),
            send_sem=far_send_sem.at[4 * t + 2 * side + sub],
            recv_sem=far_recv_sem.at[4 * t + 2 * side + sub],
            device_id={"tp": sides[side]},
            device_id_type=MESH,
        )

    def send_near(t):
        for side in range(2):
            near_copy(t, side).start()

    def take_near(t):
        for side in range(2):
            near_copy(t, side).wait_recv()

    def send_far(t, subs=(0, 1)):
        for side in range(2):
            for sub in subs:
                far_copy(t, side, sub).start()

    shared_own = (sgate_ref, sup_ref, sdown_ref)
    shared_all = (sgate_all, sup_all, sdown_all)

    crew = min(8, groups)
    seat = lax.rem(me, crew)
    stops = crew // 2
    turn = core * stops + lax.div(seat, 2)

    def half_of(t, who):
        h = shared_own[t].shape[0] // 2
        return pl.ds(pl.multiple_of(who * h, 16), h)

    def share_of(t):
        e = shared_own[t].shape[0] // crew
        return pl.ds(pl.multiple_of(turn * e, 16), e)

    def shared_near(t, side):
        return pltpu.make_async_remote_copy(
            src_ref=shared_own[t].at[share_of(t)],
            dst_ref=shared_all[t].at[side, share_of(t)],
            send_sem=near_send_sem.at[20 + 2 * t + side],
            recv_sem=near_recv_sem.at[20 + 2 * t + side],
            device_id={"tp": sides[side]},
            device_id_type=MESH,
        )

    def part_of(t, k, side):
        if t < 2:
            e = shared_own[t].shape[0] // crew
            start = pl.multiple_of(turn * e + side * (e // 2), 16)
            return shared_all[t].at[k, pl.ds(start, e // 2)]
        return shared_all[t].at[k, share_of(t), pl.ds(side * half_width, half_width)]

    def shared_far(t, side):
        return pltpu.make_async_remote_copy(
            src_ref=part_of(t, side, side),
            dst_ref=part_of(t, 2, side),
            send_sem=far_send_sem.at[40 + 2 * t + side],
            recv_sem=far_recv_sem.at[40 + 2 * t + side],
            device_id={"tp": sides[side]},
            device_id_type=MESH,
        )

    def cross_copy(t, k, n):
        return pltpu.make_async_remote_copy(
            src_ref=shared_all[t].at[k, share_of(t)],
            dst_ref=shared_all[t].at[k, share_of(t)],
            send_sem=cross_send_sem.at[(3 * t + k) * stops + n],
            recv_sem=cross_recv_sem.at[(3 * t + k) * stops + n],
            device_id={"sp": me - seat + lax.rem(seat + 2 * n, crew)},
            device_id_type=MESH,
        )

    def send_cross(k):
        for t in range(3):
            for n in range(1, stops):
                cross_copy(t, k, n).start()

    def twin_copy(t, k, part):
        return pltpu.make_async_remote_copy(
            src_ref=shared_all[t].at[k, part],
            dst_ref=shared_all[t].at[k, part],
            send_sem=twin_send_sem.at[3 * t + k],
            recv_sem=twin_recv_sem.at[3 * t + k],
            device_id={"sp": twin},
            device_id_type=MESH,
        )

    lane = lax.broadcasted_iota(jnp.int32, (CHUNK, LANES), 1)
    r_id = lax.broadcasted_iota(jnp.int32, (CHUNK, CHUNK), 0)
    c_id = lax.broadcasted_iota(jnp.int32, (CHUNK, CHUNK), 1)
    lower = r_id >= c_id
    upper = r_id <= c_id
    lower_one = jnp.where(lower, 1.0, 0.0).astype(BF16)
    upper_one = jnp.where(upper, 1.0, 0.0).astype(BF16)
    front = (lane % KEY_CHANNELS) < (KEY_CHANNELS // 2)
    first_head = lane < KEY_CHANNELS
    cos_0 = outer_ref[me, 0:1, :]
    sin_0 = outer_ref[me, 1:2, :]

    def log_decay(x):
        return (jnp.minimum(x, 0.0) - jnp.log1p(jnp.exp(-jnp.abs(x)))) * (1.0 / GATE_NORM)

    def cumulate(tri, x):
        high = x.astype(BF16)
        low = (x - high.astype(F32)).astype(BF16)
        return jnp.dot(tri, high, preferred_element_type=F32) + jnp.dot(
            tri, low, preferred_element_type=F32
        )

    pl.semaphore_wait(barrier, groups - 1 + members - 1)
    for t in range(3):
        for side in range(2):
            shared_near(t, side).start()
    send_near(0)

    for b in range(chunks):
        rows = slice(b * CHUNK, (b + 1) * CHUNK)
        cos_i = inner_ref[0, rows, :]
        sin_i = inner_ref[1, rows, :]
        cosine = cos_0 * cos_i - sin_0 * sin_i
        sine = sin_0 * cos_i + cos_0 * sin_i
        sine = jnp.where(front, -sine, sine)

        def rotated(u):
            swapped = jnp.where(
                front,
                pltpu.roll(u, LANES - KEY_CHANNELS // 2, 1),
                pltpu.roll(u, KEY_CHANNELS // 2, 1),
            )
            return u * cosine + swapped * sine

        q = rotated(q_ref[rows, :].astype(F32) * KEY_CHANNELS ** (-0.5))
        k = rotated(k_ref[rows, :].astype(F32))
        cf = cumulate(lower_one, log_decay(fd_ref[rows, :]))
        cb = cumulate(upper_one, log_decay(bd_ref[rows, :]))
        hf = cf[CHUNK - 1 : CHUNK, :] * 0.5
        hb = cb[0:1, :] * 0.5
        half_ref[2 * b : 2 * b + 1, :] = hf
        half_ref[2 * b + 1 : 2 * b + 2, :] = hb
        qf = q * jnp.exp(cf - hf)
        qb = q * jnp.exp(cb - hb)
        kf = (k * jnp.exp(hf - cf)).astype(BF16)
        kb = (k * jnp.exp(hb - cb)).astype(BF16)
        ks_ref[b, :, 0:LANES] = kf
        ks_ref[b, :, LANES : 2 * LANES] = kb
        qs_ref[b, 0:CHUNK, 0:LANES] = jnp.where(first_head, qf, 0.0).astype(BF16)
        qs_ref[b, 0:CHUNK, LANES : 2 * LANES] = jnp.where(first_head, qb, 0.0).astype(BF16)
        qs_ref[b, CHUNK : 2 * CHUNK, 0:LANES] = jnp.where(first_head, 0.0, qf).astype(BF16)
        qs_ref[b, CHUNK : 2 * CHUNK, LANES : 2 * LANES] = jnp.where(first_head, 0.0, qb).astype(
            BF16
        )
        both = lax.dot_general(
            v_ref[rows, :], ks_ref[b], TN, preferred_element_type=F32
        )
        upd_ref[2 * b] = jnp.where(
            first_head, both[0:DV, 0:LANES], both[DV : 2 * DV, 0:LANES]
        ) * jnp.exp(hf)
        upd_ref[2 * b + 1] = jnp.where(
            first_head, both[0:DV, LANES : 2 * LANES], both[DV : 2 * DV, LANES : 2 * LANES]
        ) * jnp.exp(hb)

    def decay_of(b, d):
        return jnp.exp(half_ref[2 * b + d : 2 * b + d + 1, :] * 2.0)

    total_f = upd_ref[0]
    decay_f = decay_of(0, 0)
    for b in range(1, chunks):
        total_f = total_f * decay_of(b, 0) + upd_ref[2 * b]
        decay_f = decay_f * decay_of(b, 0)
    total_b = upd_ref[2 * (chunks - 1) + 1]
    decay_b = decay_of(chunks - 1, 1)
    for b in reversed(range(chunks - 1)):
        total_b = total_b * decay_of(b, 1) + upd_ref[2 * b + 1]
        decay_b = decay_b * decay_of(b, 1)
    for r in range(share):
        part = slice(r * groups, (r + 1) * groups)
        send_ref[pl.ds(r, groups, stride=message), :] = total_f[part, :]
        send_ref[pl.ds(share + r, groups, stride=message), :] = total_b[part, :]
        send_ref[pl.ds(2 * share + r, groups, stride=message), :] = jnp.broadcast_to(
            decay_f, (groups, LANES)
        )
        send_ref[pl.ds(3 * share + r, groups, stride=message), :] = jnp.broadcast_to(
            decay_b, (groups, LANES)
        )

    def block(ref, i):
        return ref.at[pl.ds(pl.multiple_of(i * message, message), message)]

    def half_block(ref, i):
        return ref.at[i]

    def out_copy(peer, i):
        return pltpu.make_async_remote_copy(
            src_ref=block(send_ref, peer),
            dst_ref=block(got_ref, me),
            send_sem=send_sem.at[i],
            recv_sem=recv_sem.at[i],
            device_id={"sp": peer},
            device_id_type=MESH,
        )

    def back_copy(peer, i):
        return pltpu.make_async_remote_copy(
            src_ref=half_block(back_state_ref, peer),
            dst_ref=half_block(carry_ref, me),
            send_sem=back_send_sem.at[i],
            recv_sem=back_recv_sem.at[i],
            device_id={"sp": peer},
            device_id_type=MESH,
        )

    def offset(i):
        half = lax.div(i + 1, 2)
        return jnp.where(lax.rem(i, 2) == 1, half, groups - half)

    def peer_of(i):
        return lax.rem(me + offset(i), groups)

    def each(action):
        def step(i, c):
            action(i)
            return c

        lax.fori_loop(1, groups, step, 0)

    each(lambda i: out_copy(peer_of(i), offset(i)).start())
    for t in range(3):
        for side in range(2):
            shared_near(t, side).wait_recv()
            shared_far(t, side).start()
    send_cross(0)
    mine = pl.ds(pl.multiple_of(me * message, message), message)
    got_ref[mine, :] = send_ref[mine, :]

    for b in range(chunks):
        rows = slice(b * CHUNK, (b + 1) * CHUNK)
        s_f = lax.dot_general(
            qs_ref[b, :, 0:LANES], ks_ref[b, :, 0:LANES], NT, preferred_element_type=F32
        )
        s_b = lax.dot_general(
            qs_ref[b, :, LANES : 2 * LANES],
            ks_ref[b, :, LANES : 2 * LANES],
            NT,
            preferred_element_type=F32,
        )
        for h in range(2):
            part = slice(h * CHUNK, (h + 1) * CHUNK)
            s = jnp.where(lower, s_f[part], 0.0) + jnp.where(upper, s_b[part], 0.0)
            out_ref[h, rows, :] = jnp.dot(
                s.astype(BF16), v_ref[rows, h * DV : (h + 1) * DV], preferred_element_type=F32
            )

    each(lambda i: out_copy(peer_of(i), offset(i)).wait())

    zero = jnp.zeros((share, LANES), F32)

    def scan(s, carried):
        c_f, c_b = carried
        t = groups - 1 - s
        at_s = pl.multiple_of(s * message, message)
        at_t = pl.multiple_of(t * message, message)
        m_s = got_ref[pl.ds(at_s, message), :]
        m_t = got_ref[pl.ds(at_t, message), :]
        back_state_ref[s, 0:share, :] = c_f
        back_state_ref[t, share : 2 * share, :] = c_b
        c_f = c_f * m_s[2 * share : 3 * share] + m_s[0:share]
        c_b = c_b * m_t[3 * share : 4 * share] + m_t[share : 2 * share]
        return c_f, c_b

    lax.fori_loop(0, groups, scan, (zero, zero))
    each(lambda i: back_copy(peer_of(i), offset(i)).start())
    carry_ref[me] = back_state_ref[me]
    send_cross(1)
    take_near(0)
    send_far(0, (0,))
    each(lambda i: back_copy(peer_of(i), offset(i)).wait())

    state_f = jnp.concatenate([carry_ref[:, r, :] for r in range(share)], axis=0)
    state_b = jnp.concatenate([carry_ref[:, share + r, :] for r in range(share)], axis=0)
    for b in range(chunks):
        before = state_f
        mine_ref[b, :, 0:LANES] = (
            before * jnp.exp(half_ref[2 * b : 2 * b + 1, :])
        ).astype(BF16)
        state_f = state_f * decay_of(b, 0) + upd_ref[2 * b]
    for b in reversed(range(chunks)):
        mine_ref[b, :, LANES : 2 * LANES] = (
            state_b * jnp.exp(half_ref[2 * b + 1 : 2 * b + 2, :])
        ).astype(BF16)
        state_b = state_b * decay_of(b, 1) + upd_ref[2 * b + 1]

    def mix_copy(i):
        peer = lax.rem(row + i, members)
        return pltpu.make_async_remote_copy(
            src_ref=ks_ref.at[peer],
            dst_ref=mixed_ref.at[row],
            send_sem=mix_send_sem.at[i],
            recv_sem=mix_recv_sem.at[i],
            device_id={"tp": peer},
            device_id_type=MESH,
        )

    for b in range(chunks):
        rows = slice(b * CHUNK, (b + 1) * CHUNK)
        across = lax.dot_general(qs_ref[b], mine_ref[b], NT, preferred_element_type=F32)
        for h in range(2):
            o = out_ref[h, rows, :] + across[h * CHUNK : (h + 1) * CHUNK]
            cols = slice(h * DV, (h + 1) * DV)
            o = o * lax.rsqrt(jnp.mean(o * o, axis=-1, keepdims=True) + EPS)
            g = g_ref[rows, cols].astype(F32)
            o = o * gain_ref[0:1, cols] * (g / (1.0 + jnp.exp(-g)))
            ks_ref[b, :, cols] = o.astype(BF16)
    for i in range(1, members):
        mix_copy(i).start()
    for t in range(1, EARLY):
        send_near(t)
    send_far(0, (1,))
    for t in range(3):
        for side in range(2):
            shared_far(t, side).wait_recv()
    send_cross(2)
    mixed_ref[row] = ks_ref[row]

    expert_id = lax.broadcasted_iota(jnp.int32, (LANES, count), 0)
    earlier_id = lax.broadcasted_iota(jnp.int32, (count, count), 0)
    token_id = lax.broadcasted_iota(jnp.int32, (count, count), 1)
    first_named = routes_ref[0:1, :] == expert_id
    second_named = routes_ref[1:2, :] == expert_id
    named = jnp.where(first_named, 1.0, 0.0) + jnp.where(second_named, 1.0, 0.0)
    earlier = jnp.where(earlier_id < token_id, 1.0, 0.0).astype(BF16)
    rank = jnp.dot(named.astype(BF16), earlier, preferred_element_type=F32)
    ranked = (named * (rank + 1.0)).astype(BF16)
    spread = jnp.dot(spread_ref[...], ranked, preferred_element_type=F32)
    put_ref[...] = jnp.where(spread == target_ref[...], 1.0, 0.0).astype(BF16)

    local_copies[0].wait()
    for i in range(1, members):
        mix_copy(i).wait()
    mixed = jnp.concatenate([mixed_ref[i] for i in range(members)], axis=1)
    step = min(512, width)
    for n in range(width // step):
        cols = slice(n * step, (n + 1) * step)
        total_ref[:, cols] = jnp.dot(mixed, proj_ref[:, cols], preferred_element_type=F32)
    for i in range(count // 16):
        rows = slice(i * 16, (i + 1) * 16)
        p = total_ref[rows, :]
        p = p * lax.rsqrt(jnp.mean(p * p, axis=-1, keepdims=True) + EPS) * mix_gain_ref[...]
        r = (stream_ref[rows, :].astype(F32) + p).astype(BF16)
        residual_ref[rows, :] = r
        r = r.astype(F32)
        r = r * lax.rsqrt(jnp.mean(r * r, axis=-1, keepdims=True) + EPS) * ffn_gain_ref[...]
        normed_ref[rows, :] = r.astype(BF16)

    def piece_of(part, i):
        first, number = part
        piece = slots * number // groups
        return pl.ds(pl.multiple_of(slots * first + i * piece, 8), piece)

    def row_copy(src, dst, sem, part, i):
        peer = peer_of(i)
        return pltpu.make_async_remote_copy(
            src_ref=src.at[piece_of(part, peer)],
            dst_ref=dst.at[piece_of(part, me)],
            send_sem=row_send_sem.at[sem, offset(i)],
            recv_sem=row_recv_sem.at[sem, offset(i)],
            device_id={"sp": peer},
            device_id_type=MESH,
        )

    def fill_rows(part, left, right):
        first, number = part
        for n in range(number // 2):
            cols = pl.ds((first + 2 * n) * LANES, 2 * LANES)
            f = jnp.dot(left[...], right[:, cols], preferred_element_type=F32)
            for k in range(2):
                at = pl.ds(slots * first + 2 * n + k, slots, stride=number)
                stage_ref[at, :] = f[:, k * LANES : (k + 1) * LANES]

        def one(i, c):
            filled_ref[piece_of(part, i), :] = stage_ref[piece_of(part, i), :].astype(BF16)
            return c

        lax.fori_loop(0, groups, one, 0)

    def get_lines(dst, part):
        first, number = part
        for k in range(number):
            at = pl.ds(slots * first + k, slots, stride=number)
            n = first + k
            dst[:, n * LANES : (n + 1) * LANES] = stage_ref[at, :].astype(BF16)

    def send_rows(dst, sem, part):
        each(lambda i: row_copy(filled_ref, dst, sem, part, i).start())

    def take_rows(dst, sem, part):
        own = piece_of(part, me)
        stage_ref[own, :] = filled_ref[own, :].astype(F32)

        def one(i):
            row_copy(filled_ref, dst, sem, part, i).wait()
            came = piece_of(part, lax.rem(me + groups - offset(i), groups))
            stage_ref[came, :] = dst[came, :].astype(F32)

        each(one)

    for sem, part in enumerate(OUT_PARTS):
        fill_rows(part, put_ref, normed_ref)
        send_rows(arrived_ref, sem, part)

    def shared(gate, up, down, first):
        x = normed_ref[...]
        g = jnp.dot(x, gate[...], preferred_element_type=F32)
        u = jnp.dot(x, up[...], preferred_element_type=F32)
        h = (g / (1.0 + jnp.exp(-g)) * u).astype(BF16)
        for n in range(width // step):
            cols = slice(n * step, (n + 1) * step)
            more = jnp.dot(h, down[:, cols], preferred_element_type=F32)
            if first:
                total_ref[:, cols] = more
            else:
                total_ref[:, cols] += more

    for t in range(3):
        for k in range(3):
            for n in range(1, stops):
                cross_copy(t, k, n).wait_recv()
            twin_copy(t, k, half_of(t, core)).start()
    take_near(1)
    send_far(1)
    take_near(2)
    send_far(2)
    for t in range(EARLY, 2 + len(BACK_PARTS)):
        send_near(t)
    for t in range(3, EARLY):
        take_near(t)
        send_far(t)
    shared(sgate_ref, sup_ref, sdown_ref, True)
    for k in range(3):
        for t in range(3):
            twin_copy(t, k, half_of(t, 1 - core)).wait_recv()
        shared(sgate_all.at[k], sup_all.at[k], sdown_all.at[k], False)
    for sem, part in enumerate(OUT_PARTS):
        take_rows(arrived_ref, sem, part)
    for part in OUT_PARTS:
        get_lines(x_ref, part)
    for copy in local_copies[1:]:
        copy.wait()

    def hide(slot):
        g = jnp.dot(x_ref[...], gate_all[slot], preferred_element_type=F32)
        u = jnp.dot(x_ref[...], up_all[slot], preferred_element_type=F32)
        hidden_ref[:, slot * inner_width : (slot + 1) * inner_width] = (
            g / (1.0 + jnp.exp(-g)) * u
        ).astype(BF16)

    for slot in range(3):
        hide(slot)
    for t in range(2):
        for side in range(2):
            for sub in range(2):
                far_copy(t, side, sub).wait_recv()
    hide(3)
    sent = EARLY
    for n, part in enumerate(BACK_PARTS):
        if 2 + n >= sent:
            take_near(2 + n)
            send_far(2 + n)
        for side in range(2):
            for sub in range(2):
                far_copy(2 + n, side, sub).wait_recv()
        fill_rows(part, hidden_ref, down_all)
        send_rows(back_ref, len(OUT_PARTS) + n, part)

    first_weight = jnp.where(first_named, weight_ref[0:1, :], 0.0)
    weigh = first_weight + jnp.where(second_named, weight_ref[1:2, :], 0.0)
    high = weigh.astype(BF16)
    low = (weigh - high.astype(F32)).astype(BF16)
    put = put_ref[...].astype(F32)
    high = (jnp.dot(spread_ref[...], high, preferred_element_type=F32) * put).astype(BF16)
    low = (jnp.dot(spread_ref[...], low, preferred_element_type=F32) * put).astype(BF16)

    for t in range(2 + len(BACK_PARTS)):
        for side in range(2):
            near_copy(t, side).wait_send()
            for sub in range(2):
                far_copy(t, side, sub).wait_send()
    for t in range(3):
        for side in range(2):
            shared_near(t, side).wait_send()
            shared_far(t, side).wait_send()
        for k in range(3):
            for n in range(1, stops):
                cross_copy(t, k, n).wait_send()
            twin_copy(t, k, half_of(t, core)).wait_send()

    for n, part in enumerate(BACK_PARTS):
        take_rows(back_ref, len(OUT_PARTS) + n, part)
        get_lines(x_ref, part)
        for k in range(part[1] // 2):
            cols = pl.ds((part[0] + 2 * k) * LANES, 2 * LANES)
            total_ref[:, cols] += lax.dot_general(
                high, x_ref[:, cols], TN, preferred_element_type=F32
            ) + lax.dot_general(low, x_ref[:, cols], TN, preferred_element_type=F32)
    for i in range(count // 16):
        rows = slice(i * 16, (i + 1) * 16)
        m = total_ref[rows, :]
        m = m * lax.rsqrt(jnp.mean(m * m, axis=-1, keepdims=True) + EPS) * moe_gain_ref[...]
        updated_ref[rows, :] = (residual_ref[rows, :].astype(F32) + m).astype(BF16)


def slot_tables(experts):
    slot = np.arange(experts * CAP)
    spread = (slot[:, None] // CAP == np.arange(LANES)[None, :]).astype(np.float32)
    target = (slot % CAP + 1).astype(np.float32).reshape(-1, 1)
    return spread, target


def body(
    mesh,
    stream,
    queries,
    key_rows,
    values,
    out_gate,
    fwd_decay,
    bwd_decay,
    head_gain,
    out_proj,
    mix_gain,
    ffn_gain,
    moe_gain,
    routes,
    route_weight,
    expert_gate,
    expert_up,
    expert_down,
    shared_gate,
    shared_up,
    shared_down,
):
    groups, members = mesh.shape["sp"], mesh.shape["tp"]
    span = queries.shape[0]
    chunks = span // CHUNK
    share = DV // groups
    tokens, width = stream.shape
    slots = groups * CAP
    lines = width // LANES
    inner_width = expert_gate.shape[2]
    inner, outer = rope_tables(span, groups)
    spread, target = slot_tables(groups)
    vmem = pl.BlockSpec(memory_space=pltpu.VMEM)
    anywhere = pl.BlockSpec(memory_space=pl.ANY)
    dma = pltpu.SemaphoreType.DMA
    mem = pltpu.VMEM
    return pl.pallas_call(
        functools.partial(layer_kernel, groups, members),
        out_shape=jax.ShapeDtypeStruct((tokens, width), BF16),
        in_specs=[vmem] * 20 + [anywhere] * 4,
        out_specs=vmem,
        scratch_shapes=[
            mem(out_proj.shape, BF16),
            mem((members, width, inner_width), BF16),
            mem((members, width, inner_width), BF16),
            mem((members * inner_width, width), BF16),
            mem((3, *shared_gate.shape), BF16),
            mem((3, *shared_up.shape), BF16),
            mem((3, *shared_down.shape), BF16),
            mem((members, CHUNK, 2 * DV), BF16),
            mem((tokens, width), F32),
            mem((tokens, width), BF16),
            mem((tokens, width), BF16),
            mem((slots, tokens), BF16),
            mem((slots * lines, LANES), F32),
            mem((slots * lines, LANES), BF16),
            mem((slots * lines, LANES), BF16),
            mem((slots * lines, LANES), BF16),
            mem((slots, width), BF16),
            mem((slots, members * inner_width), BF16),
            mem((chunks, 2 * CHUNK, 2 * LANES), BF16),
            mem((chunks, CHUNK, 2 * LANES), BF16),
            mem((2, span, DV), F32),
            mem((2 * chunks, DV, LANES), F32),
            mem((2 * chunks, LANES), F32),
            mem((groups * 4 * share, LANES), F32),
            mem((groups * 4 * share, LANES), F32),
            mem((groups, 2 * share, LANES), F32),
            mem((groups, 2 * share, LANES), F32),
            mem((chunks, DV, 2 * LANES), BF16),
            dma((groups,)),
            dma((groups,)),
            dma((groups,)),
            dma((groups,)),
            dma((members,)),
            dma((members,)),
            dma((len(OUT_PARTS) + len(BACK_PARTS), groups)),
            dma((len(OUT_PARTS) + len(BACK_PARTS), groups)),
            dma((26,)),
            dma((26,)),
            dma((46,)),
            dma((46,)),
            dma((9 * min(4, groups // 2),)),
            dma((9 * min(4, groups // 2),)),
            dma((9,)),
            dma((9,)),
            dma((4,)),
        ],
        compiler_params=pltpu.CompilerParams(
            collective_id=0, has_side_effects=True, vmem_limit_bytes=60 * 2**20
        ),
        cost_estimate=pl.CostEstimate(flops=10**10, bytes_accessed=10**8, transcendentals=0),
        name="layer",
    )(
        queries,
        key_rows,
        values,
        out_gate,
        fwd_decay,
        bwd_decay,
        head_gain.reshape(1, -1),
        jnp.asarray(inner),
        jnp.asarray(outer),
        stream,
        mix_gain.reshape(1, -1),
        ffn_gain.reshape(1, -1),
        moe_gain.reshape(1, -1),
        routes.T,
        route_weight.T,
        jnp.asarray(spread).astype(BF16),
        jnp.asarray(target),
        shared_gate,
        shared_up,
        shared_down,
        out_proj,
        expert_gate[0],
        expert_up[0],
        expert_down[0],
    )


def solution(mesh):
    placed = (
        P(("sp", "tp"), None),
        P("sp", "tp"),
        P("sp", "tp"),
        P("sp", "tp"),
        P("sp", "tp"),
        P("sp", "tp"),
        P("sp", "tp"),
        P("tp"),
        P(),
        P(),
        P(),
        P(),
        P(("sp", "tp"), None),
        P(("sp", "tp"), None),
        P("sp", None, "tp"),
        P("sp", None, "tp"),
        P("sp", "tp", None),
        P(None, "tp"),
        P(None, "tp"),
        P("tp", None),
    )
    return jax.shard_map(
        functools.partial(body, mesh),
        mesh=mesh,
        in_specs=placed,
        out_specs=P(("sp", "tp"), None),
        check_vma=False,
    )
```
